256 devices in a mesh: sp: 64 (over z, x, core), tp: 4 (over y).
Axes of the slice: x: 4, y: 4, z: 8, core: 2. Of those that a mesh axis runs over, the one named last changes fastest.
Arguments:
- residual: bfloat16 [16384, 2048], P(('sp', 'tp')), may hold values from -6 to 6
- first_query: bfloat16 [16384, 512], P('sp', 'tp'), may hold values from -6 to 6
- second_query: bfloat16 [16384, 512], P('sp', 'tp'), may hold values from -6 to 6
- first_key: bfloat16 [16384, 512], P('sp', 'tp'), may hold values from -6 to 6
- second_key: bfloat16 [16384, 512], P('sp', 'tp'), may hold values from -6 to 6
- values: bfloat16 [16384, 1024], P('sp', 'tp'), may hold values from -6 to 6
- lambdas: float32 [8], P('tp'), may hold values from 0.3 to 0.8
- head_gain: float32 [128], replicated, may hold values from 0.1 to 1.9
- out_weight: bfloat16 [1024, 2048], P('tp'), may hold values from -0.1875 to 0.1875
- norm_gain: float32 [2048], replicated, may hold values from 0.1 to 1.9
- up_weight: bfloat16 [2048, 4096], P('sp', 'tp'), may hold values from -0.125 to 0.125
- down_weight: bfloat16 [4096, 2048], P('tp', 'sp'), may hold values from -0.09375 to 0.09375
Outputs:
- mixed: bfloat16 [16384, 2048], P(('sp', 'tp'))
The draws below stay inside these ranges and needn't reach their ends.
All inputs are finite; a program needn't handle non-finite values.
Results may differ from the reference program's by a relative error of at most 0.019.
Values may be sent and summed in bfloat16 or wider, within the bound.
No kernel may reach another device: no remote copies, remote signals or barrier semaphores. Data moves between devices by JAX's collectives and lax.ppermute only.
A program may use at most 128 MiB of HBM per device.

```python
import jax
import jax.numpy as jnp
from jax import lax

D = 2048
HEADS = 8
HEAD = 64
VDIM = 128
FF = 4096
TOK_DEV = 256
TOKENS = 16384


def draw_entries(key, which_map, which_role):
    own_key = jax.random.fold_in(key, 100 * which_map + which_role)
    width = HEADS * HEAD
    data = jnp.clip(1.3 * jax.random.normal(own_key, (TOKENS, width), jnp.float32), -6.0, 6.0)
    return data.astype(jnp.bfloat16)


def draw_first_query(key, part):
    return draw_entries(key, 1, 0)


def draw_first_key(key, part):
    return draw_entries(key, 1, 1)


def draw_second_query(key, part):
    return draw_entries(key, 2, 0)


def draw_second_key(key, part):
    return draw_entries(key, 2, 1)


def steps_of(key, shape, split, least, top_value):
    level, own = 1.0, jax.random.fold_in(key, 6)
    for axis_at, blocks in split:
        heights = jnp.exp(jax.random.uniform(jax.random.fold_in(own, axis_at), (blocks,), jnp.float32, least / len(split), top_value / len(split)))
        level = level * jnp.repeat(heights, shape[axis_at] // blocks).reshape([-1 if axis == axis_at else 1 for axis in range(len(shape))])
    return level


def gaussian(key, dims, scale, most, shards=(), held_as=jnp.bfloat16):
    result = jax.random.normal(key, dims, jnp.float32) * scale
    if len(shards) > 0:
        result = steps_of(key, dims, shards, -0.22, 0.18) * result
    return jnp.clip(result, min=-most, max=most).astype(held_as)


def setup_inputs(seed: int = 0) -> dict:
    arg_keys = jax.random.split(jax.random.key(seed), 13)
    residual = gaussian(arg_keys[0], (TOKENS, D), 1.0, 6.0, ((0, 256),))
    first_query = draw_first_query(jax.random.fold_in(arg_keys[12], 71), 0)
    second_query = draw_second_query(jax.random.fold_in(arg_keys[12], 71), 0)
    first_key = draw_first_key(jax.random.fold_in(arg_keys[12], 71), 0)
    second_key = draw_second_key(jax.random.fold_in(arg_keys[12], 71), 0)
    values = gaussian(arg_keys[5], (TOKENS, HEADS * VDIM), 1.0, 6.0, ((0, 64), (1, 4)))
    lambdas = jnp.clip(0.3 + 0.5 * jax.random.uniform(arg_keys[6], (HEADS,), jnp.float32) ** steps_of(arg_keys[6], (HEADS,), ((0, 4),), -0.2, 0.2), 0.3, 0.8)
    head_gain = jnp.clip(1.0 + 0.18 * jax.random.normal(arg_keys[7], (VDIM,), jnp.float32), 0.1, 1.9)
    out_weight = gaussian(arg_keys[8], (HEADS * VDIM, D), (HEADS * VDIM) ** -0.5, 0.1875, ((0, 4),))
    norm_gain = jnp.clip(1.0 + 0.18 * jax.random.normal(arg_keys[9], (D,), jnp.float32), 0.1, 1.9)
    up_weight = gaussian(arg_keys[10], (D, FF), D ** -0.5, 0.125, ((0, 64), (1, 4)))
    down_weight = gaussian(arg_keys[11], (FF, D), FF ** -0.5, 0.09375, ((0, 4), (1, 64)))
    return dict(residual=residual, first_query=first_query, second_query=second_query, first_key=first_key, second_key=second_key, values=values, lambdas=lambdas, head_gain=head_gain, out_weight=out_weight, norm_gain=norm_gain, up_weight=up_weight, down_weight=down_weight)


def rotate(blocked, positions):
    half = blocked.shape[-1] // 2
    inverse = 10000.0 ** (-jnp.arange(0, half, dtype=jnp.float32) * 2.0 / blocked.shape[-1])
    angle = positions[:, None] * inverse[None, :]
    cosine = jnp.cos(angle)[:, None, :]
    sine = jnp.sin(angle)[:, None, :]
    first, second = (blocked[..., :half], blocked[..., half:])
    return jnp.concatenate([first * cosine - second * sine, second * cosine + first * sine], axis=-1)

def attend(queries, keys, vals):
    scores = jnp.dot(queries, keys.T, preferred_element_type=jnp.float32) * HEAD ** (-0.5)
    peak = lax.optimization_barrier(jnp.max(scores, axis=-1, keepdims=True))
    weights = jnp.exp(scores - peak)
    total = lax.optimization_barrier(jnp.sum(weights, axis=-1, keepdims=True))
    summed = jnp.dot(weights.astype(jnp.bfloat16), vals, preferred_element_type=jnp.float32)
    return summed / total

def layer_norm(stream, gain):
    center = stream - lax.optimization_barrier(jnp.mean(stream, axis=-1, keepdims=True))
    spread = lax.optimization_barrier(jnp.mean(center * center, axis=-1, keepdims=True))
    return center * lax.rsqrt(spread + 1e-05) * gain

def reference(residual, first_query, second_query, first_key, second_key, values, lambdas, head_gain, out_weight, norm_gain, up_weight, down_weight):
    length = residual.shape[0]
    positions = jnp.arange(length, dtype=jnp.float32)

    def prepare(source):
        turned = rotate(source.astype(jnp.float32).reshape(length, HEADS, HEAD), positions)
        return turned.astype(jnp.bfloat16).transpose(1, 0, 2)
    query_a, query_b = (prepare(first_query), prepare(second_query))
    key_a, key_b = (prepare(first_key), prepare(second_key))
    vals = values.reshape(length, HEADS, VDIM).transpose(1, 0, 2)

    def one_head(item):
        part_a, part_b, keys_a, keys_b, head_vals, weight = item

        def one_block(pair):
            return attend(pair[0], keys_a, head_vals) - weight * attend(pair[1], keys_b, head_vals)
        blocks = lax.map(one_block, (part_a.reshape(-1, TOK_DEV, HEAD), part_b.reshape(-1, TOK_DEV, HEAD)))
        return blocks.reshape(length, VDIM)
    diff = lax.map(one_head, (query_a, query_b, key_a, key_b, vals, lambdas))
    scale = lax.rsqrt(lax.optimization_barrier(jnp.mean(diff * diff, axis=-1, keepdims=True)) + 1e-05)
    heads_out = (diff * scale * head_gain * 0.8).astype(jnp.bfloat16)
    flat = heads_out.transpose(1, 0, 2).reshape(length, HEADS * VDIM)
    projected = jnp.dot(flat, out_weight, preferred_element_type=jnp.float32)
    normed = layer_norm(residual.astype(jnp.float32) + projected, norm_gain).astype(jnp.bfloat16)
    lifted = jnp.dot(normed, up_weight, preferred_element_type=jnp.float32)
    hidden = jnp.square(jax.nn.relu(lifted)).astype(jnp.bfloat16)
    lowered = jnp.dot(hidden, down_weight, preferred_element_type=jnp.float32)
    return (normed.astype(jnp.float32) + lowered).astype(jnp.bfloat16)
```

```python
import jax
import jax.numpy as jnp
from jax import lax
from jax.experimental import pallas as pl
from jax.experimental.pallas import tpu as pltpu
from jax.sharding import Mesh, PartitionSpec as P

F32 = jnp.float32
BF16 = jnp.bfloat16
TOK = 256
HEAD = 64
VD = 128
LOG2E = 1.4426950408889634
NT = (((1,), (1,)), ((), ()))
NN = (((1,), (0,)), ((), ()))
ANY = pl.BlockSpec(memory_space=pl.ANY)
SMEM = pl.BlockSpec(memory_space=pltpu.SMEM)
VMEM = pl.BlockSpec(memory_space=pltpu.VMEM)
WIDE = 5 * VD


def prep_kernel(cos_ref, sin_ref, qa_ref, qb_ref, ka_ref, kb_ref, v_ref, q_out, kv_out):
    cos = cos_ref[...]
    sin = sin_ref[...]
    lane = lax.broadcasted_iota(jnp.int32, cos.shape, 1)
    front = (lane % HEAD) < HEAD // 2

    def turn(ref):
        x = ref[...].astype(F32)
        other = jnp.where(front, pltpu.roll(x, 128 - 32, 1), pltpu.roll(x, 32, 1))
        return (x * cos + other * sin).astype(BF16)

    q_out[:, 0:128] = turn(qa_ref)
    q_out[:, 128:256] = turn(qb_ref)
    kv_out[0:TOK, 0:128] = turn(ka_ref)
    kv_out[0:TOK, 128:256] = turn(kb_ref)
    kv_out[TOK : 2 * TOK, :] = v_ref[...].astype(F32).T.astype(BF16)


def prepare(first_query, second_query, first_key, second_key, values, start):
    positions = (start + jnp.arange(TOK)).astype(F32)
    half = HEAD // 2
    inverse = 10000.0 ** (-jnp.arange(0, half, dtype=F32) * 2.0 / HEAD)
    angle = positions[:, None] * inverse[None, :]
    cos, sin = jnp.cos(angle), jnp.sin(angle)
    cos4 = jnp.concatenate([cos] * 4, axis=1)
    sin4 = jnp.concatenate([-sin, sin, -sin, sin], axis=1)
    return pl.pallas_call(
        prep_kernel,
        out_shape=(
            jax.ShapeDtypeStruct((TOK, 2 * VD), BF16),
            jax.ShapeDtypeStruct((2 * TOK, 2 * VD), BF16),
        ),
        in_specs=[VMEM] * 7,
        out_specs=(VMEM, VMEM),
        name="prep",
    )(cos4, sin4, first_query, second_query, first_key, second_key, values)


def three_parts(value):
    hi = value.astype(BF16).astype(F32)
    rest = value - hi
    mid = rest.astype(BF16).astype(F32)
    return hi, mid, rest - mid


GROUP = 4


def attend_kernel(x_ref, lam_ref, q0, q1, q2, q3, kv_ref, out_ref, qs, sc, acc, top, tot, stat):
    lane = lax.broadcasted_iota(jnp.int32, (TOK, 128), 1)
    for o, q in enumerate((q0, q1, q2, q3)):
        for m in range(2):
            scaled = q[:, m * 128 : (m + 1) * 128].astype(F32) * (LOG2E * HEAD**-0.5)
            hi = scaled.astype(BF16).astype(F32)
            lo = scaled - hi
            for h in range(2):
                mine = (lane < HEAD) if h == 0 else (lane >= HEAD)
                qs[o, 2 * h + m, :, 0:128] = jnp.where(mine, hi, 0.0).astype(BF16)
                qs[o, 2 * h + m, :, 128:256] = jnp.where(mine, lo, 0.0).astype(BF16)
    top[...] = jnp.full_like(top, -1e30)
    tot[...] = jnp.zeros_like(tot)
    acc[...] = jnp.zeros_like(acc)

    def scores(slot, group, o, hm):
        m = hm % 2
        keys = kv_ref[pl.ds(group * GROUP, GROUP), 0:TOK, m * 128 : (m + 1) * 128]
        keys = keys.reshape(GROUP * TOK, 128)
        both = jnp.concatenate([keys, keys], axis=1)
        sc[slot] = lax.dot_general(both, qs[o, hm], NT, preferred_element_type=F32)

    groups = kv_ref.shape[0] // GROUP
    scores(0, 0, 0, 0)

    def step(i, carry):
        group, o = i // 4, i % 4
        after = jnp.minimum(i + 1, groups * 4 - 1)
        for hm in range(4):
            if hm < 3:
                scores((hm + 1) % 2, group, o, hm + 1)
            else:
                scores(0, after // 4, after % 4, 0)
            h = hm // 2
            s = sc[hm % 2]
            old = top[o, hm]
            new = jnp.maximum(old, jnp.max(s, axis=0, keepdims=True))
            shrink = jnp.exp2(old - new)
            p = jnp.exp2(s - new)
            top[o, hm] = new
            tot[o, hm] = tot[o, hm] * shrink + jnp.sum(p, axis=0, keepdims=True)
            vals = jnp.concatenate(
                [kv_ref[group * GROUP + g, TOK + h * VD : TOK + (h + 1) * VD, :] for g in range(GROUP)],
                axis=1,
            )
            acc[o, hm] = acc[o, hm] * shrink + lax.dot_general(
                vals, p.astype(BF16), NN, preferred_element_type=F32
            )
        return carry

    lax.fori_loop(0, groups * 4, step, 0)
    stat[...] = jnp.zeros_like(stat)
    for h in range(2):
        for i, part in enumerate(three_parts(jnp.full((1, TOK), lam_ref[h], F32))):
            stat[12 + 3 * h + i : 13 + 3 * h + i, :] = part
    for o in range(4):
        home = (x_ref[0] + 4 - o) % 4
        for hm in range(4):
            total = tot[o, hm]
            out_ref[home, :, hm * VD : (hm + 1) * VD] = (acc[o, hm] / total).T.astype(BF16)
            for i, part in enumerate(three_parts(top[o, hm] + jnp.log2(total))):
                stat[3 * hm + i : 3 * hm + i + 1, :] = part
        out_ref[home, :, 4 * VD :] = stat[...].T.astype(BF16)


def attend(x, lambdas, queries, kv):
    return pl.pallas_call(
        attend_kernel,
        out_shape=jax.ShapeDtypeStruct((4, TOK, WIDE), BF16),
        in_specs=[SMEM, SMEM] + [VMEM] * 5,
        out_specs=VMEM,
        scratch_shapes=[
            pltpu.VMEM((4, 4, TOK, 256), BF16),
            pltpu.VMEM((2, GROUP * TOK, TOK), F32),
            pltpu.VMEM((4, 4, VD, TOK), F32),
            pltpu.VMEM((4, 4, 1, TOK), F32),
            pltpu.VMEM((4, 4, 1, TOK), F32),
            pltpu.VMEM((VD, TOK), F32),
        ],
        compiler_params=pltpu.CompilerParams(vmem_limit_bytes=40 * 2**20),
        name="attend",
    )(x, lambdas, *queries, kv)


def merge_kernel(y_ref, part_ref, gain_ref, res_ref, norm_ref, w0, w1, w2, w3, out_ref, wbuf, sem):
    copies = [
        pltpu.make_async_copy(w, wbuf.at[o], sem.at[o]) for o, w in enumerate((w0, w1, w2, w3))
    ]
    for copy in copies:
        copy.start()
    stream = res_ref[...].astype(F32)
    for o in range(4):
        y = (y_ref[0] + 4 - o) % 4
        parts = [part_ref[4 * k + y] for k in range(4)]
        stats = [p[:, 4 * VD :].astype(F32) for p in parts]
        heads = []
        for h in range(2):
            maps = []
            for m in range(2):
                hm = 2 * h + m
                at = 3 * hm
                lse = [s[:, at : at + 1] + s[:, at + 1 : at + 2] + s[:, at + 2 : at + 3] for s in stats]
                peak = jnp.maximum(jnp.maximum(lse[0], lse[1]), jnp.maximum(lse[2], lse[3]))
                share = [jnp.exp2(e - peak) for e in lse]
                inv = 1.0 / (share[0] + share[1] + share[2] + share[3])
                maps.append(
                    sum(
                        p[:, hm * VD : (hm + 1) * VD].astype(F32) * (w * inv)
                        for p, w in zip(parts, share)
                    )
                )
            at = 12 + 3 * h
            lam = stats[0][:, at : at + 1] + stats[0][:, at + 1 : at + 2] + stats[0][:, at + 2 : at + 3]
            diff = maps[0] - lam * maps[1]
            scale = lax.rsqrt(jnp.mean(diff * diff, axis=-1, keepdims=True) + 1e-05)
            heads.append((diff * scale * gain_ref[...] * 0.8).astype(BF16))
        flat = jnp.concatenate(heads, axis=1)
        copies[o].wait()
        stream = stream + lax.dot_general(flat, wbuf[o], NN, preferred_element_type=F32)
    center = stream - jnp.mean(stream, axis=-1, keepdims=True)
    spread = jnp.mean(center * center, axis=-1, keepdims=True)
    out_ref[...] = (center * lax.rsqrt(spread + 1e-05) * norm_ref[...]).astype(BF16)


def merge(y, part, head_gain, residual, norm_gain, weights):
    rows, width = residual.shape
    return pl.pallas_call(
        merge_kernel,
        out_shape=jax.ShapeDtypeStruct((rows, width), BF16),
        in_specs=[SMEM] + [VMEM] * 4 + [ANY] * 4,
        out_specs=VMEM,
        scratch_shapes=[pltpu.VMEM((4, 2 * VD, width), BF16), pltpu.SemaphoreType.DMA((4,))],
        compiler_params=pltpu.CompilerParams(vmem_limit_bytes=24 * 2**20),
        name="merge",
    )(y, part, head_gain.reshape(1, VD), residual, norm_gain.reshape(1, width), *weights)


def mixer_kernel(n0, n1, n2, n3, w_ref, o0, o1, o2, o3, up, down, sem):
    cuts = 4
    per = up.shape[0] // cuts
    copies = []
    for side, buf in enumerate((up, down)):
        for i in range(cuts):
            at = pl.ds(i * per, per)
            copies.append(pltpu.make_async_copy(w_ref.at[at, side], buf.at[at], sem.at[side * cuts + i]))
            copies[-1].start()
    hidden_width = up.shape[2]
    step = per * up.shape[1]
    x = jnp.concatenate([n[...] for n in (n0, n1, n2, n3)], axis=0)
    lifted = jnp.zeros((x.shape[0], hidden_width), F32)
    for i in range(cuts):
        copies[i].wait()
        block = up[i * per : (i + 1) * per].reshape(step, hidden_width)
        lifted = lifted + lax.dot_general(
            x[:, i * step : (i + 1) * step], block, NN, preferred_element_type=F32
        )
    pos = jnp.maximum(lifted, 0.0)
    hidden = (pos * pos).astype(BF16)
    rows = n0.shape[0]
    for i in range(cuts):
        copies[cuts + i].wait()
        block = down[i * per : (i + 1) * per].reshape(step, hidden_width)
        low = lax.dot_general(hidden, block, NT, preferred_element_type=F32)
        for k, o in enumerate((o0, o1, o2, o3)):
            o[:, i * step : (i + 1) * step] = low[k * rows : (k + 1) * rows].astype(o.dtype)


def mixer(pieces, weights):
    rows, width = pieces[0].shape
    return pl.pallas_call(
        mixer_kernel,
        out_shape=[jax.ShapeDtypeStruct((rows, width), F32 if k == 0 else BF16) for k in range(4)],
        in_specs=[VMEM] * 4 + [ANY],
        out_specs=[VMEM] * 4,
        scratch_shapes=[
            pltpu.VMEM((weights.shape[0],) + weights.shape[2:], BF16),
            pltpu.VMEM((weights.shape[0],) + weights.shape[2:], BF16),
            pltpu.SemaphoreType.DMA((8,)),
        ],
        compiler_params=pltpu.CompilerParams(vmem_limit_bytes=32 * 2**20),
        name="mixer",
    )(*pieces, weights)


def shifted(value, axis, by):
    size = lax.axis_size(axis)
    return lax.ppermute(value, axis, [(i, (i + by) % size) for i in range(size)])


def local(
    residual,
    first_query,
    second_query,
    first_key,
    second_key,
    values,
    lambdas,
    head_gain,
    out_weight,
    norm_gain,
    up_weight,
    down_weight,
):
    sp = lax.axis_index(("z", "x", "c"))
    x = lax.axis_index("x").astype(jnp.int32).reshape(1)
    y = lax.axis_index("tp").astype(jnp.int32).reshape(1)
    query, kv = prepare(first_query, second_query, first_key, second_key, values, sp * TOK)
    kv_all = lax.all_gather(kv, ("z", "c"))
    both = jnp.stack([up_weight, down_weight.T])
    queries = [query] + [shifted(query, "x", o) for o in (1, 2, 3)]
    out_weights = [out_weight] + [shifted(out_weight, "tp", o) for o in (1, 2, 3)]
    mix_weights = lax.all_gather(both, ("z", "x", "c"))
    part = attend(x, lambdas, queries, kv_all)
    part = part.reshape(16, 64, WIDE)
    part = lax.all_to_all(part, ("x", "tp"), split_axis=0, concat_axis=0, tiled=True)
    normed = merge(y, part, head_gain, residual, norm_gain, out_weights)
    pieces = [normed] + [shifted(normed, "tp", o) for o in (1, 2, 3)]
    lows = mixer(pieces, mix_weights)
    total = normed.astype(F32) + lows[0]
    for o in (1, 2, 3):
        total = total + shifted(lows[o], "tp", -o).astype(F32)
    return total.astype(BF16)


def solution(mesh):
    fine = Mesh(mesh.devices.reshape(8, 4, 2, 4), ("z", "x", "c", "tp"))
    sp = ("z", "x", "c")
    in_specs = (
        P(sp + ("tp",), None),
        P(sp, "tp"),
        P(sp, "tp"),
        P(sp, "tp"),
        P(sp, "tp"),
        P(sp, "tp"),
        P("tp"),
        P(),
        P("tp", None),
        P(),
        P(sp, "tp"),
        P("tp", sp),
    )
    out_specs = P(sp + ("tp",), None)
    return jax.shard_map(local, mesh=fine, in_specs=in_specs, out_specs=out_specs, check_vma=False)
```

```python
import jax
import jax.numpy as jnp
from jax import lax
from jax.experimental import pallas as pl
from jax.experimental.pallas import tpu as pltpu
from jax.sharding import Mesh, PartitionSpec as P


F32 = jnp.float32
BF16 = jnp.bfloat16
TOK = 256
HEAD = 64
VD = 128
LOG2E = 1.4426950408889634
NT = (((1,), (1,)), ((), ()))
NN = (((1,), (0,)), ((), ()))
ANY = pl.BlockSpec(memory_space=pl.ANY)
SMEM = pl.BlockSpec(memory_space=pltpu.SMEM)
VMEM = pl.BlockSpec(memory_space=pltpu.VMEM)
WIDE = 5 * VD


def prep_kernel(cos_ref, sin_ref, qa_ref, qb_ref, ka_ref, kb_ref, v_ref, q_out, kv_out):
    cos = cos_ref[...]
    sin = sin_ref[...]
    lane = lax.broadcasted_iota(jnp.int32, cos.shape, 1)
    front = (lane % HEAD) < HEAD // 2

    def turn(ref):
        x = ref[...].astype(F32)
        other = jnp.where(front, pltpu.roll(x, 128 - 32, 1), pltpu.roll(x, 32, 1))
        return (x * cos + other * sin).astype(BF16)

    q_out[:, 0:128] = turn(qa_ref)
    q_out[:, 128:256] = turn(qb_ref)
    kv_out[0:TOK, 0:128] = turn(ka_ref)
    kv_out[0:TOK, 128:256] = turn(kb_ref)
    kv_out[TOK : 2 * TOK, :] = v_ref[...].astype(F32).T.astype(BF16)


def prepare(first_query, second_query, first_key, second_key, values, start):
    positions = (start + jnp.arange(TOK)).astype(F32)
    half = HEAD // 2
    inverse = 10000.0 ** (-jnp.arange(0, half, dtype=F32) * 2.0 / HEAD)
    angle = positions[:, None] * inverse[None, :]
    cos, sin = jnp.cos(angle), jnp.sin(angle)
    cos4 = jnp.concatenate([cos] * 4, axis=1)
    sin4 = jnp.concatenate([-sin, sin, -sin, sin], axis=1)
    return pl.pallas_call(
        prep_kernel,
        out_shape=(
            jax.ShapeDtypeStruct((TOK, 2 * VD), BF16),
            jax.ShapeDtypeStruct((2 * TOK, 2 * VD), BF16),
        ),
        in_specs=[VMEM] * 7,
        out_specs=(VMEM, VMEM),
        name="prep",
    )(cos4, sin4, first_query, second_query, first_key, second_key, values)


def three_parts(value):
    hi = value.astype(BF16).astype(F32)
    rest = value - hi
    mid = rest.astype(BF16).astype(F32)
    return hi, mid, rest - mid


def load_queries(queries, qs):
    lane = lax.broadcasted_iota(jnp.int32, (TOK, 128), 1)
    for o, q in enumerate(queries):
        for m in range(2):
            scaled = q[:, m * 128 : (m + 1) * 128].astype(F32) * (LOG2E * HEAD**-0.5)
            hi = scaled.astype(BF16).astype(F32)
            lo = scaled - hi
            for h in range(2):
                mine = (lane < HEAD) if h == 0 else (lane >= HEAD)
                qs[o, 2 * h + m, :, 0:128] = jnp.where(mine, hi, 0.0).astype(BF16)
                qs[o, 2 * h + m, :, 128:256] = jnp.where(mine, lo, 0.0).astype(BF16)


def absorb(chunks, qs, sc, acc, top, tot, fresh):
    def scores(slot, o, hm):
        m = hm % 2
        keys = jnp.concatenate([c[0:TOK, m * 128 : (m + 1) * 128] for c in chunks], axis=0)
        both = jnp.concatenate([keys, keys], axis=1)
        s = lax.dot_general(both, qs[o, hm], NT, preferred_element_type=F32)
        sc[slot] = s
        return jnp.max(s, axis=0, keepdims=True)

    def step(o, peak):
        after = jnp.minimum(o + 1, 3)
        for hm in range(4):
            here = peak
            peak = scores((hm + 1) % 2, o, hm + 1) if hm < 3 else scores(0, after, 0)
            h = hm // 2
            if fresh:
                new = here
            else:
                old = top[o, hm]
                new = jnp.maximum(old, here)
                shrink = jnp.exp2(old - new)
            p = jnp.exp2(sc[hm % 2] - new)
            vals = jnp.concatenate([c[TOK + h * VD : TOK + (h + 1) * VD, :] for c in chunks], axis=1)
            moved = lax.dot_general(vals, p.astype(BF16), NN, preferred_element_type=F32)
            total = jnp.sum(p, axis=0, keepdims=True)
            top[o, hm] = new
            if fresh:
                tot[o, hm] = total
                acc[o, hm] = moved
            else:
                tot[o, hm] = tot[o, hm] * shrink + total
                acc[o, hm] = acc[o, hm] * shrink + moved
        return peak

    lax.fori_loop(0, 4, step, scores(0, 0, 0))


def finish(x_ref, lam_ref, out_ref, stat, acc, top, tot):
    stat[...] = jnp.zeros_like(stat)
    for h in range(2):
        for i, part in enumerate(three_parts(jnp.full((1, TOK), lam_ref[h], F32))):
            stat[12 + 3 * h + i : 13 + 3 * h + i, :] = part
    for o in range(4):
        home = (x_ref[0] + 4 - o) % 4
        for hm in range(4):
            total = tot[o, hm]
            out_ref[home, :, hm * VD : (hm + 1) * VD] = (acc[o, hm] / total).T.astype(BF16)
            for i, part in enumerate(three_parts(top[o, hm] + jnp.log2(total))):
                stat[3 * hm + i : 3 * hm + i + 1, :] = part
        out_ref[home, :, 4 * VD :] = stat[...].T.astype(BF16)


STATE = (
    jax.ShapeDtypeStruct((4, 4, VD, TOK), F32),
    jax.ShapeDtypeStruct((4, 4, 1, TOK), F32),
    jax.ShapeDtypeStruct((4, 4, 1, TOK), F32),
)
QS = jax.ShapeDtypeStruct((4, 4, TOK, 2 * VD), BF16)


def chunks_of(ref):
    return [ref] if len(ref.shape) == 2 else [ref.at[i] for i in range(ref.shape[0])]


def first_kernel(q0, q1, q2, q3, own_ref, other_ref, qs, acc, top, tot, sc):
    load_queries((q0, q1, q2, q3), qs)
    absorb([own_ref, other_ref], qs, sc, acc, top, tot, True)


def next_kernel(qs, kv_ref, acc_in, top_in, tot_in, acc, top, tot, sc):
    absorb(chunks_of(kv_ref), qs, sc, acc, top, tot, False)


def last_kernel(x_ref, lam_ref, qs, kv_ref, acc_in, top_in, tot_in, out_ref, acc, top, tot, sc, stat):
    acc[...] = acc_in[...]
    top[...] = top_in[...]
    tot[...] = tot_in[...]
    absorb(chunks_of(kv_ref), qs, sc, acc, top, tot, False)
    finish(x_ref, lam_ref, out_ref, stat, acc, top, tot)


def cost(keys):
    return pl.CostEstimate(
        flops=2 * keys * 4 * TOK * 4 * 3 * HEAD,
        bytes_accessed=keys * 1024,
        transcendentals=keys * 4 * TOK * 4,
    )


def score_scratch(chunks):
    return pltpu.VMEM((2, chunks * TOK, TOK), F32)


def attend_first(queries, own, other):
    return pl.pallas_call(
        first_kernel,
        out_shape=(QS,) + STATE,
        in_specs=[VMEM] * 6,
        out_specs=(VMEM,) * 4,
        scratch_shapes=[score_scratch(2)],
        cost_estimate=cost(512),
        compiler_params=pltpu.CompilerParams(vmem_limit_bytes=24 * 2**20),
        name="attend_first",
    )(*queries, own, other)


def attend_next(qs, kv, state):
    return pl.pallas_call(
        next_kernel,
        out_shape=STATE,
        in_specs=[VMEM] * 5,
        out_specs=(VMEM,) * 3,
        input_output_aliases={2: 0, 3: 1, 4: 2},
        scratch_shapes=[score_scratch(kv.shape[0])],
        cost_estimate=cost(kv.shape[0] * TOK),
        compiler_params=pltpu.CompilerParams(vmem_limit_bytes=24 * 2**20),
        name="attend_next",
    )(qs, kv, *state)


def attend_last(x, lambdas, qs, kv, state):
    return pl.pallas_call(
        last_kernel,
        out_shape=jax.ShapeDtypeStruct((4, TOK, WIDE), BF16),
        in_specs=[SMEM, SMEM] + [VMEM] * 5,
        out_specs=VMEM,
        scratch_shapes=[pltpu.VMEM(s.shape, s.dtype) for s in STATE]
        + [score_scratch(kv.shape[0]), pltpu.VMEM((VD, TOK), F32)],
        cost_estimate=cost(kv.shape[0] * TOK),
        compiler_params=pltpu.CompilerParams(vmem_limit_bytes=24 * 2**20),
        name="attend_last",
    )(x, lambdas, qs, kv, *state)


def merge_kernel(y_ref, part_ref, gain_ref, res_ref, norm_ref, w0, w1, w2, w3, out_ref, wbuf, sem):
    copies = [
        pltpu.make_async_copy(w, wbuf.at[o], sem.at[o]) for o, w in enumerate((w0, w1, w2, w3))
    ]
    for copy in copies:
        copy.start()
    stream = res_ref[...].astype(F32)
    for o in range(4):
        y = (y_ref[0] + 4 - o) % 4
        parts = [part_ref[4 * k + y] for k in range(4)]
        stats = [p[:, 4 * VD :].astype(F32) for p in parts]
        heads = []
        for h in range(2):
            maps = []
            for m in range(2):
                hm = 2 * h + m
                at = 3 * hm
                lse = [s[:, at : at + 1] + s[:, at + 1 : at + 2] + s[:, at + 2 : at + 3] for s in stats]
                peak = jnp.maximum(jnp.maximum(lse[0], lse[1]), jnp.maximum(lse[2], lse[3]))
                share = [jnp.exp2(e - peak) for e in lse]
                inv = 1.0 / (share[0] + share[1] + share[2] + share[3])
                maps.append(
                    sum(
                        p[:, hm * VD : (hm + 1) * VD].astype(F32) * (w * inv)
                        for p, w in zip(parts, share)
                    )
                )
            at = 12 + 3 * h
            lam = stats[0][:, at : at + 1] + stats[0][:, at + 1 : at + 2] + stats[0][:, at + 2 : at + 3]
            diff = maps[0] - lam * maps[1]
            scale = lax.rsqrt(jnp.mean(diff * diff, axis=-1, keepdims=True) + 1e-05)
            heads.append((diff * scale * gain_ref[...] * 0.8).astype(BF16))
        flat = jnp.concatenate(heads, axis=1)
        copies[o].wait()
        stream = stream + lax.dot_general(flat, wbuf[o], NN, preferred_element_type=F32)
    center = stream - jnp.mean(stream, axis=-1, keepdims=True)
    spread = jnp.mean(center * center, axis=-1, keepdims=True)
    out_ref[...] = (center * lax.rsqrt(spread + 1e-05) * norm_ref[...]).astype(BF16)


def merge(y, part, head_gain, residual, norm_gain, weights):
    rows, width = residual.shape
    return pl.pallas_call(
        merge_kernel,
        out_shape=jax.ShapeDtypeStruct((rows, width), BF16),
        in_specs=[SMEM] + [VMEM] * 4 + [ANY] * 4,
        out_specs=VMEM,
        scratch_shapes=[pltpu.VMEM((4, 2 * VD, width), BF16), pltpu.SemaphoreType.DMA((4,))],
        compiler_params=pltpu.CompilerParams(vmem_limit_bytes=24 * 2**20),
        name="merge",
    )(y, part, head_gain.reshape(1, VD), residual, norm_gain.reshape(1, width), *weights)


def mixer_kernel(n0, n1, n2, n3, w_ref, o0, o1, o2, o3, up, down, sem):
    cuts = 4
    per = up.shape[0] // cuts
    copies = []
    for side, buf in enumerate((up, down)):
        for i in range(cuts):
            at = pl.ds(i * per, per)
            copies.append(pltpu.make_async_copy(w_ref.at[at, side], buf.at[at], sem.at[side * cuts + i]))
            copies[-1].start()
    hidden_width = up.shape[2]
    step = per * up.shape[1]
    x = jnp.concatenate([n[...] for n in (n0, n1, n2, n3)], axis=0)
    lifted = jnp.zeros((x.shape[0], hidden_width), F32)
    for i in range(cuts):
        copies[i].wait()
        block = up[i * per : (i + 1) * per].reshape(step, hidden_width)
        lifted = lifted + lax.dot_general(
            x[:, i * step : (i + 1) * step], block, NN, preferred_element_type=F32
        )
    pos = jnp.maximum(lifted, 0.0)
    hidden = (pos * pos).astype(BF16)
    rows = n0.shape[0]
    for i in range(cuts):
        copies[cuts + i].wait()
        block = down[i * per : (i + 1) * per].reshape(step, hidden_width)
        low = lax.dot_general(hidden, block, NT, preferred_element_type=F32)
        for k, o in enumerate((o0, o1, o2, o3)):
            o[:, i * step : (i + 1) * step] = low[k * rows : (k + 1) * rows].astype(o.dtype)


def mixer(pieces, weights):
    rows, width = pieces[0].shape
    return pl.pallas_call(
        mixer_kernel,
        out_shape=[jax.ShapeDtypeStruct((rows, width), F32 if k == 0 else BF16) for k in range(4)],
        in_specs=[VMEM] * 4 + [ANY],
        out_specs=[VMEM] * 4,
        scratch_shapes=[
            pltpu.VMEM((weights.shape[0],) + weights.shape[2:], BF16),
            pltpu.VMEM((weights.shape[0],) + weights.shape[2:], BF16),
            pltpu.SemaphoreType.DMA((8,)),
        ],
        compiler_params=pltpu.CompilerParams(vmem_limit_bytes=32 * 2**20),
        name="mixer",
    )(*pieces, weights)


def shifted(value, axis, by):
    size = lax.axis_size(axis)
    return lax.ppermute(value, axis, [(i, (i + by) % size) for i in range(size)])


def local(
    residual,
    first_query,
    second_query,
    first_key,
    second_key,
    values,
    lambdas,
    head_gain,
    out_weight,
    norm_gain,
    up_weight,
    down_weight,
):
    sp = lax.axis_index(("z", "x", "c"))
    x = lax.axis_index("x").astype(jnp.int32).reshape(1)
    y = lax.axis_index("tp").astype(jnp.int32).reshape(1)
    query, kv = prepare(first_query, second_query, first_key, second_key, values, sp * TOK)
    ring = ("z", "c")
    onward = [(2 * z + c, 2 * ((z + 1 - 2 * c) % 8) + c) for z in range(8) for c in range(2)]
    crossed = [(2 * z + c, 2 * ((z - 1 + 2 * c) % 8) + 1 - c) for z in range(8) for c in range(2)]
    near = [lax.ppermute(kv, ring, onward), lax.ppermute(kv, ring, crossed)]
    other = shifted(kv, "c", 1)
    queries = [query] + [shifted(query, "x", o) for o in (1, 2, 3)]
    mix_weights = jnp.stack([up_weight, down_weight.T])
    mix_weights = lax.all_gather(mix_weights, ("z", "x", "c"))
    near = jnp.stack(near)
    second = lax.ppermute(near, ring, onward)
    qs, *state = attend_first(queries, kv, other)
    out_weights = [out_weight] + [shifted(out_weight, "tp", o) for o in (1, 2, 3)]
    third = lax.ppermute(second, ring, onward)
    four = jnp.concatenate([near, second])
    four_other = shifted(four, "c", 1)
    state = attend_next(qs, four, state)
    far = lax.ppermute(third[0], ring, onward)
    state = attend_next(qs, four_other, state)
    three = jnp.concatenate([third, far[None]])
    three_other = shifted(three, "c", 1)
    state = attend_next(qs, three, state)
    part = attend_last(x, lambdas, qs, three_other, state)
    part = part.reshape(16, 64, WIDE)
    part = lax.all_to_all(part, ("x", "tp"), split_axis=0, concat_axis=0, tiled=True)
    normed = merge(y, part, head_gain, residual, norm_gain, out_weights)
    pieces = [normed] + [shifted(normed, "tp", o) for o in (1, 2, 3)]
    lows = mixer(pieces, mix_weights)
    total = normed.astype(F32) + lows[0]
    for o in (1, 2, 3):
        total = total + shifted(lows[o], "tp", -o).astype(F32)
    return total.astype(BF16)


def solution(mesh):
    fine = Mesh(mesh.devices.reshape(8, 4, 2, 4), ("z", "x", "c", "tp"))
    sp = ("z", "x", "c")
    in_specs = (
        P(sp + ("tp",), None),
        P(sp, "tp"),
        P(sp, "tp"),
        P(sp, "tp"),
        P(sp, "tp"),
        P(sp, "tp"),
        P("tp"),
        P(),
        P("tp", None),
        P(),
        P(sp, "tp"),
        P("tp", sp),
    )
    out_specs = P(sp + ("tp",), None)

    return jax.shard_map(local, mesh=fine, in_specs=in_specs, out_specs=out_specs, check_vma=False)
```

```python
import functools

import jax
import jax.numpy as jnp
from jax import lax
from jax.experimental import pallas as pl
from jax.experimental.pallas import tpu as pltpu
from jax.sharding import Mesh, PartitionSpec as P


F32 = jnp.float32
BF16 = jnp.bfloat16
TOK = 256
HEAD = 64
VD = 128
LOG2E = 1.4426950408889634
NT = (((1,), (1,)), ((), ()))
NN = (((1,), (0,)), ((), ()))
ANY = pl.BlockSpec(memory_space=pl.ANY)
SMEM = pl.BlockSpec(memory_space=pltpu.SMEM)
VMEM = pl.BlockSpec(memory_space=pltpu.VMEM)
WIDE = 5 * VD


def prep_kernel(cos_ref, sin_ref, qa_ref, qb_ref, ka_ref, kb_ref, v_ref, q_out, kv_out, q_own, kv_own):
    cos = cos_ref[...]
    sin = sin_ref[...]
    lane = lax.broadcasted_iota(jnp.int32, cos.shape, 1)
    front = (lane % HEAD) < HEAD // 2

    def turn(ref):
        x = ref[...].astype(F32)
        other = jnp.where(front, pltpu.roll(x, 128 - 32, 1), pltpu.roll(x, 32, 1))
        return (x * cos + other * sin).astype(BF16)

    q_out[:, 0:128] = turn(qa_ref)
    q_out[:, 128:256] = turn(qb_ref)
    kv_out[0:TOK, 0:128] = turn(ka_ref)
    kv_out[0:TOK, 128:256] = turn(kb_ref)
    kv_out[TOK : 2 * TOK, :] = v_ref[...].astype(F32).T.astype(BF16)
    q_own[...] = q_out[...]
    kv_own[...] = kv_out[...]


def prepare(first_query, second_query, first_key, second_key, values, start):
    positions = (start + jnp.arange(TOK)).astype(F32)
    half = HEAD // 2
    inverse = 10000.0 ** (-jnp.arange(0, half, dtype=F32) * 2.0 / HEAD)
    angle = positions[:, None] * inverse[None, :]
    cos, sin = jnp.cos(angle), jnp.sin(angle)
    cos4 = jnp.concatenate([cos] * 4, axis=1)
    sin4 = jnp.concatenate([-sin, sin, -sin, sin], axis=1)
    return pl.pallas_call(
        prep_kernel,
        out_shape=(
            jax.ShapeDtypeStruct((TOK, 2 * VD), BF16),
            jax.ShapeDtypeStruct((2 * TOK, 2 * VD), BF16),
        )
        * 2,
        in_specs=[VMEM] * 7,
        out_specs=(VMEM,) * 4,
        name="prep",
    )(cos4, sin4, first_query, second_query, first_key, second_key, values)


def three_parts(value):
    hi = value.astype(BF16).astype(F32)
    rest = value - hi
    mid = rest.astype(BF16).astype(F32)
    return hi, mid, rest - mid


def load_queries(queries, qs):
    lane = lax.broadcasted_iota(jnp.int32, (TOK, 128), 1)
    for o, q in enumerate(queries):
        for m in range(2):
            scaled = q[:, m * 128 : (m + 1) * 128].astype(F32) * (LOG2E * HEAD**-0.5)
            hi = scaled.astype(BF16).astype(F32)
            lo = scaled - hi
            for h in range(2):
                mine = (lane < HEAD) if h == 0 else (lane >= HEAD)
                qs[o, 2 * h + m, :, 0:128] = jnp.where(mine, hi, 0.0).astype(BF16)
                qs[o, 2 * h + m, :, 128:256] = jnp.where(mine, lo, 0.0).astype(BF16)


def absorb(chunks, qs, sc, acc, top, tot, fresh):
    def scores(slot, o, hm):
        m = hm % 2
        keys = jnp.concatenate([c[0:TOK, m * 128 : (m + 1) * 128] for c in chunks], axis=0)
        both = jnp.concatenate([keys, keys], axis=1)
        s = lax.dot_general(both, qs[o, hm], NT, preferred_element_type=F32)
        sc[slot] = s
        return jnp.max(s, axis=0, keepdims=True)

    def step(o, peak):
        after = jnp.minimum(o + 1, 3)
        for hm in range(4):
            here = peak
            peak = scores((hm + 1) % 2, o, hm + 1) if hm < 3 else scores(0, after, 0)
            h = hm // 2
            if fresh:
                new = here
            else:
                old = top[o, hm]
                new = jnp.maximum(old, here)
                shrink = jnp.exp2(old - new)
            p = jnp.exp2(sc[hm % 2] - new)
            vals = jnp.concatenate([c[TOK + h * VD : TOK + (h + 1) * VD, :] for c in chunks], axis=1)
            moved = lax.dot_general(vals, p.astype(BF16), NN, preferred_element_type=F32)
            total = jnp.sum(p, axis=0, keepdims=True)
            top[o, hm] = new
            if fresh:
                tot[o, hm] = total
                acc[o, hm] = moved
            else:
                tot[o, hm] = tot[o, hm] * shrink + total
                acc[o, hm] = acc[o, hm] * shrink + moved
        return peak

    lax.fori_loop(0, 4, step, scores(0, 0, 0))


def finish(x_ref, lam_ref, out_ref, stat, acc, top, tot):
    stat[...] = jnp.zeros_like(stat)
    for h in range(2):
        for i, part in enumerate(three_parts(jnp.full((1, TOK), lam_ref[h], F32))):
            stat[12 + 3 * h + i : 13 + 3 * h + i, :] = part
    for o in range(4):
        home = (x_ref[0] + 4 - o) % 4
        for hm in range(4):
            total = tot[o, hm]
            out_ref[home, :, hm * VD : (hm + 1) * VD] = (acc[o, hm] / total).T.astype(BF16)
            for i, part in enumerate(three_parts(top[o, hm] + jnp.log2(total))):
                stat[3 * hm + i : 3 * hm + i + 1, :] = part
        out_ref[home, :, 4 * VD :] = stat[...].T.astype(BF16)


STATE = (
    jax.ShapeDtypeStruct((4, 4, VD, TOK), F32),
    jax.ShapeDtypeStruct((4, 4, 1, TOK), F32),
    jax.ShapeDtypeStruct((4, 4, 1, TOK), F32),
)
QS = jax.ShapeDtypeStruct((4, 4, TOK, 2 * VD), BF16)


def chunks_of(ref):
    return [ref] if len(ref.shape) == 2 else [ref.at[i] for i in range(ref.shape[0])]


def first_kernel(q0, q1, q2, q3, own_ref, other_ref, qs, acc, top, tot, sc):
    load_queries((q0, q1, q2, q3), qs)
    absorb([own_ref, other_ref], qs, sc, acc, top, tot, True)


def next_kernel(qs, kv_ref, acc_in, top_in, tot_in, acc, top, tot, sc):
    absorb(chunks_of(kv_ref), qs, sc, acc, top, tot, False)


def last_kernel(x_ref, lam_ref, qs, kv_ref, acc_in, top_in, tot_in, out_ref, acc, top, tot, sc, stat):
    acc[...] = acc_in[...]
    top[...] = top_in[...]
    tot[...] = tot_in[...]
    absorb(chunks_of(kv_ref), qs, sc, acc, top, tot, False)
    finish(x_ref, lam_ref, out_ref, stat, acc, top, tot)


def cost(keys):
    return pl.CostEstimate(
        flops=2 * keys * 4 * TOK * 4 * 3 * HEAD,
        bytes_accessed=keys * 1024,
        transcendentals=keys * 4 * TOK * 4,
    )


def score_scratch(chunks):
    return pltpu.VMEM((2, chunks * TOK, TOK), F32)


def attend_first(queries, own, other):
    return pl.pallas_call(
        first_kernel,
        out_shape=(QS,) + STATE,
        in_specs=[VMEM] * 6,
        out_specs=(VMEM,) * 4,
        scratch_shapes=[score_scratch(2)],
        cost_estimate=cost(512),
        compiler_params=pltpu.CompilerParams(vmem_limit_bytes=24 * 2**20),
        name="attend_first",
    )(*queries, own, other)


def attend_next(qs, kv, state):
    return pl.pallas_call(
        next_kernel,
        out_shape=STATE,
        in_specs=[VMEM] * 5,
        out_specs=(VMEM,) * 3,
        input_output_aliases={2: 0, 3: 1, 4: 2},
        scratch_shapes=[score_scratch(kv.shape[0])],
        cost_estimate=cost(kv.shape[0] * TOK),
        compiler_params=pltpu.CompilerParams(vmem_limit_bytes=24 * 2**20),
        name="attend_next",
    )(qs, kv, *state)


def attend_last(x, lambdas, qs, kv, state):
    return pl.pallas_call(
        last_kernel,
        out_shape=jax.ShapeDtypeStruct((4, TOK, WIDE), BF16),
        in_specs=[SMEM, SMEM] + [VMEM] * 5,
        out_specs=VMEM,
        scratch_shapes=[pltpu.VMEM(s.shape, s.dtype) for s in STATE]
        + [score_scratch(kv.shape[0]), pltpu.VMEM((VD, TOK), F32)],
        cost_estimate=cost(kv.shape[0] * TOK),
        compiler_params=pltpu.CompilerParams(vmem_limit_bytes=24 * 2**20),
        name="attend_last",
    )(x, lambdas, qs, kv, *state)


def merge_kernel(at_ref, part_ref, gain_ref, res_ref, norm_ref, own_ref, mine_ref, other_ref, out_ref, wbuf, sem):
    copies = [[pltpu.make_async_copy(own_ref, wbuf.at[0], sem.at[0])]]
    mine = at_ref[1] * VD
    for o in range(3):
        copies.append(
            [
                pltpu.make_async_copy(mine_ref.at[o], wbuf.at[o + 1, pl.ds(mine, VD)], sem.at[2 * o + 1]),
                pltpu.make_async_copy(
                    other_ref.at[o], wbuf.at[o + 1, pl.ds(VD - mine, VD)], sem.at[2 * o + 2]
                ),
            ]
        )
    for pair in copies:
        for copy in pair:
            copy.start()
    stream = res_ref[...].astype(F32)
    for o in range(4):
        y = (at_ref[0] + 4 - o) % 4
        parts = [part_ref[4 * k + y] for k in range(4)]
        stats = [p[:, 4 * VD :].astype(F32) for p in parts]
        heads = []
        for h in range(2):
            maps = []
            for m in range(2):
                hm = 2 * h + m
                at = 3 * hm
                lse = [s[:, at : at + 1] + s[:, at + 1 : at + 2] + s[:, at + 2 : at + 3] for s in stats]
                peak = jnp.maximum(jnp.maximum(lse[0], lse[1]), jnp.maximum(lse[2], lse[3]))
                share = [jnp.exp2(e - peak) for e in lse]
                inv = 1.0 / (share[0] + share[1] + share[2] + share[3])
                maps.append(
                    sum(
                        p[:, hm * VD : (hm + 1) * VD].astype(F32) * (w * inv)
                        for p, w in zip(parts, share)
                    )
                )
            at = 12 + 3 * h
            lam = stats[0][:, at : at + 1] + stats[0][:, at + 1 : at + 2] + stats[0][:, at + 2 : at + 3]
            diff = maps[0] - lam * maps[1]
            scale = lax.rsqrt(jnp.mean(diff * diff, axis=-1, keepdims=True) + 1e-05)
            heads.append((diff * scale * gain_ref[...] * 0.8).astype(BF16))
        flat = jnp.concatenate(heads, axis=1)
        for copy in copies[o]:
            copy.wait()
        stream = stream + lax.dot_general(flat, wbuf[o], NN, preferred_element_type=F32)
    center = stream - jnp.mean(stream, axis=-1, keepdims=True)
    spread = jnp.mean(center * center, axis=-1, keepdims=True)
    out_ref[...] = (center * lax.rsqrt(spread + 1e-05) * norm_ref[...]).astype(BF16)


def merge(at, part, head_gain, residual, norm_gain, weights):
    rows, width = residual.shape
    return pl.pallas_call(
        merge_kernel,
        out_shape=jax.ShapeDtypeStruct((rows, width), BF16),
        in_specs=[SMEM] + [VMEM] * 4 + [ANY] * 3,
        out_specs=VMEM,
        scratch_shapes=[pltpu.VMEM((4, 2 * VD, width), BF16), pltpu.SemaphoreType.DMA((7,))],
        compiler_params=pltpu.CompilerParams(vmem_limit_bytes=24 * 2**20),
        name="merge",
    )(at, part, head_gain.reshape(1, VD), residual, norm_gain.reshape(1, width), *weights)


def mixer_kernel(count, *refs):
    pieces, w_ref, outs = refs[:count], refs[count], refs[count + 1 :]
    devices, _, rows, hidden_width = w_ref.shape
    x = jnp.concatenate([n[...] for n in pieces], axis=0)
    cuts = 4
    per = devices // cuts
    step = per * rows
    lifted = None
    for i in range(cuts):
        block = w_ref[i * per : (i + 1) * per, 0].reshape(step, hidden_width)
        more = lax.dot_general(x[:, i * step : (i + 1) * step], block, NN, preferred_element_type=F32)
        lifted = more if lifted is None else lifted + more
    pos = jnp.maximum(lifted, 0.0)
    hidden = (pos * pos).astype(BF16)
    for i in range(cuts):
        block = w_ref[i * per : (i + 1) * per, 1].reshape(step, hidden_width)
        low = lax.dot_general(hidden, block, NT, preferred_element_type=F32)
        at = 0
        for n, o in zip(pieces, outs):
            o[:, i * step : (i + 1) * step] = low[at : at + o.shape[0]].astype(o.dtype)
            at += o.shape[0]


def mixer(pieces, weights, types):
    width = pieces[0].shape[1]
    return pl.pallas_call(
        functools.partial(mixer_kernel, len(pieces)),
        out_shape=[jax.ShapeDtypeStruct(n.shape, t) for n, t in zip(pieces, types)],
        in_specs=[VMEM] * (len(pieces) + 1),
        out_specs=[VMEM] * len(pieces),
        cost_estimate=pl.CostEstimate(flops=2 * 256 * width * 2048, bytes_accessed=2**23, transcendentals=0),
        compiler_params=pltpu.CompilerParams(vmem_limit_bytes=24 * 2**20),
        name="mixer",
    )(*pieces, weights)


def shifted(value, axis, by):
    size = lax.axis_size(axis)
    return lax.ppermute(value, axis, [(i, (i + by) % size) for i in range(size)])


def local(
    residual,
    first_query,
    second_query,
    first_key,
    second_key,
    values,
    lambdas,
    head_gain,
    out_weight,
    norm_gain,
    up_weight,
    down_weight,
):
    sp = lax.axis_index(("z", "x", "c"))
    x = lax.axis_index("x").astype(jnp.int32).reshape(1)
    at = jnp.stack([lax.axis_index("tp"), lax.axis_index("c")]).astype(jnp.int32)
    query, kv, query_own, kv_own = prepare(first_query, second_query, first_key, second_key, values, sp * TOK)
    ring = ("z", "c")
    onward = [(2 * z + c, 2 * ((z + 1 - 2 * c) % 8) + c) for z in range(8) for c in range(2)]
    crossed = [(2 * z + c, 2 * ((z - 1 + 2 * c) % 8) + 1 - c) for z in range(8) for c in range(2)]
    near = [lax.ppermute(kv, ring, onward), lax.ppermute(kv, ring, crossed)]
    other = shifted(kv, "c", 1)
    queries = [query_own] + [shifted(query, "x", o) for o in (1, 2, 3)]
    mix_weights = jnp.stack([up_weight, down_weight.T])
    mix_weights = lax.all_gather(mix_weights, ("z", "x", "c"))
    half = lax.dynamic_slice_in_dim(out_weight, lax.axis_index("c") * VD, VD, 0)
    near = jnp.stack(near)
    second = lax.ppermute(near, ring, onward)
    mine = jnp.stack([shifted(half, "tp", o) for o in (1, 2, 3)])
    out_weights = [out_weight, mine, shifted(mine, "c", 1)]
    qs, *state = attend_first(queries, kv_own, other)
    third = lax.ppermute(second, ring, onward)
    four = jnp.concatenate([near, second])
    four_other = shifted(four, "c", 1)
    state = attend_next(qs, four, state)
    far = lax.ppermute(third[0], ring, onward)
    state = attend_next(qs, four_other, state)
    three = jnp.concatenate([third, far[None]])
    three_other = shifted(three, "c", 1)
    state = attend_next(qs, three, state)
    part = attend_last(x, lambdas, qs, three_other, state)
    part = part.reshape(16, 64, WIDE)
    part = lax.all_to_all(part, ("x", "tp"), split_axis=0, concat_axis=0, tiled=True)
    normed = merge(at, part, head_gain, residual, norm_gain, out_weights)
    rows = normed.shape[0] // 2
    before = shifted(normed, "tp", 1)
    after = shifted(normed, "tp", -1)
    cut1 = before[:rows]
    cut3 = after[rows:]
    across1 = shifted(cut1, "tp", 1)
    across3 = shifted(cut3, "tp", -1)
    low0, low1, low3 = mixer([normed, before, after], mix_weights, (F32, BF16, BF16))
    low1 = shifted(low1, "tp", -1)
    low3 = shifted(low3, "tp", 1)
    across = jnp.concatenate([across1, across3])
    (low2,) = mixer([across], mix_weights, (BF16,))
    low2 = shifted(low2, "tp", 2)
    total = normed.astype(F32) + low0
    for low in (low1, low2, low3):
        total = total + low.astype(F32)
    return total.astype(BF16)


def solution(mesh):
    fine = Mesh(mesh.devices.reshape(8, 4, 2, 4), ("z", "x", "c", "tp"))
    sp = ("z", "x", "c")
    in_specs = (
        P(sp + ("tp",), None),
        P(sp, "tp"),
        P(sp, "tp"),
        P(sp, "tp"),
        P(sp, "tp"),
        P(sp, "tp"),
        P("tp"),
        P(),
        P("tp", None),
        P(),
        P(sp, "tp"),
        P("tp", sp),
    )
    out_specs = P(sp + ("tp",), None)

    return jax.shard_map(local, mesh=fine, in_specs=in_specs, out_specs=out_specs, check_vma=False)
```

```python
import functools

import jax
import jax.numpy as jnp
from jax import lax
from jax.experimental import pallas as pl
from jax.experimental.pallas import tpu as pltpu
from jax.sharding import Mesh, PartitionSpec as P


F32 = jnp.float32
BF16 = jnp.bfloat16
TOK = 256
HEAD = 64
VD = 128
LOG2E = 1.4426950408889634
NT = (((1,), (1,)), ((), ()))
NN = (((1,), (0,)), ((), ()))
HBM = pl.BlockSpec(memory_space=pltpu.HBM)
SMEM = pl.BlockSpec(memory_space=pltpu.SMEM)
VMEM = pl.BlockSpec(memory_space=pltpu.VMEM)
WIDE = 5 * VD


def prep_kernel(cos_ref, sin_ref, qa_ref, qb_ref, ka_ref, kb_ref, v_ref, q_out, kv_out, q_own, kv_own):
    cos = jnp.concatenate([cos_ref[...]] * 4, axis=1)
    sin = jnp.concatenate([-sin_ref[...], sin_ref[...]] * 2, axis=1)
    lane = lax.broadcasted_iota(jnp.int32, cos.shape, 1)
    front = (lane % HEAD) < HEAD // 2

    def turn(ref):
        x = ref[...].astype(F32)
        other = jnp.where(front, pltpu.roll(x, 128 - 32, 1), pltpu.roll(x, 32, 1))
        return (x * cos + other * sin).astype(BF16)

    q_out[:, 0:128] = turn(qa_ref)
    q_out[:, 128:256] = turn(qb_ref)
    kv_out[0:TOK, 0:128] = turn(ka_ref)
    kv_out[0:TOK, 128:256] = turn(kb_ref)
    kv_out[TOK : 2 * TOK, :] = v_ref[...].astype(F32).T.astype(BF16)
    q_own[...] = q_out[...]
    kv_own[...] = kv_out[...]


def prepare(first_query, second_query, first_key, second_key, values, start):
    positions = (start + jnp.arange(TOK)).astype(F32)
    half = HEAD // 2
    inverse = 10000.0 ** (-jnp.arange(0, half, dtype=F32) * 2.0 / HEAD)
    angle = positions[:, None] * inverse[None, :]
    cos, sin = jnp.cos(angle), jnp.sin(angle)
    return pl.pallas_call(
        prep_kernel,
        out_shape=(
            jax.ShapeDtypeStruct((TOK, 2 * VD), BF16),
            jax.ShapeDtypeStruct((2 * TOK, 2 * VD), BF16),
        )
        * 2,
        in_specs=[VMEM] * 7,
        out_specs=(VMEM,) * 4,
        name="prep",
    )(cos, sin, first_query, second_query, first_key, second_key, values)


def three_parts(value):
    hi = value.astype(BF16).astype(F32)
    rest = value - hi
    mid = rest.astype(BF16).astype(F32)
    return hi, mid, rest - mid


def load_queries(queries, qs):
    lane = lax.broadcasted_iota(jnp.int32, (TOK, 128), 1)
    for o, q in enumerate(queries):
        for m in range(2):
            scaled = q[:, m * 128 : (m + 1) * 128].astype(F32) * (LOG2E * HEAD**-0.5)
            hi = scaled.astype(BF16).astype(F32)
            lo = scaled - hi
            for h in range(2):
                mine = (lane < HEAD) if h == 0 else (lane >= HEAD)
                qs[o, 2 * h + m, :, 0:128] = jnp.where(mine, hi, 0.0).astype(BF16)
                qs[o, 2 * h + m, :, 128:256] = jnp.where(mine, lo, 0.0).astype(BF16)


def absorb(chunks, qs, sc, acc, top, tot, fresh, block_done=None):
    def scores(slot, o, hm):
        m = hm % 2
        keys = jnp.concatenate([c[0:TOK, m * 128 : (m + 1) * 128] for c in chunks], axis=0)
        both = jnp.concatenate([keys, keys], axis=1)
        s = lax.dot_general(both, qs[o, hm], NT, preferred_element_type=F32)
        sc[slot] = s
        return jnp.max(s, axis=0, keepdims=True)

    def step(o, peak):
        after = jnp.minimum(o + 1, 3)
        for hm in range(4):
            here = peak
            peak = scores((hm + 1) % 2, o, hm + 1) if hm < 3 else scores(0, after, 0)
            h = hm // 2
            if fresh:
                new = here
            else:
                old = top[o, hm]
                new = jnp.maximum(old, here)
                shrink = jnp.exp2(old - new)
            p = jnp.exp2(sc[hm % 2] - new)
            vals = jnp.concatenate([c[TOK + h * VD : TOK + (h + 1) * VD, :] for c in chunks], axis=1)
            moved = lax.dot_general(vals, p.astype(BF16), NN, preferred_element_type=F32)
            total = jnp.sum(p, axis=0, keepdims=True)
            top[o, hm] = new
            if fresh:
                tot[o, hm] = total
                acc[o, hm] = moved
            else:
                tot[o, hm] = tot[o, hm] * shrink + total
                acc[o, hm] = acc[o, hm] * shrink + moved
        if block_done is not None:
            block_done(o)
        return peak

    lax.fori_loop(0, 4, step, scores(0, 0, 0))


STATE = (
    jax.ShapeDtypeStruct((4, 4, VD, TOK), F32),
    jax.ShapeDtypeStruct((4, 4, 1, TOK), F32),
    jax.ShapeDtypeStruct((4, 4, 1, TOK), F32),
)
QS = jax.ShapeDtypeStruct((4, 4, TOK, 2 * VD), BF16)


def chunks_of(ref):
    return [ref] if len(ref.shape) == 2 else [ref.at[i] for i in range(ref.shape[0])]


def first_kernel(q0, q1, q2, q3, own_ref, other_ref, qs, acc, top, tot, sc):
    load_queries((q0, q1, q2, q3), qs)
    absorb([own_ref, other_ref], qs, sc, acc, top, tot, True)


def next_kernel(qs, kv_ref, acc_in, top_in, tot_in, acc, top, tot, sc):
    absorb(chunks_of(kv_ref), qs, sc, acc, top, tot, False)


def last_kernel(
    x_ref, lam_ref, qs, kv_ref, acc_in, top_in, tot_in, out_ref, acc, top, tot, sc, stat, buf, sem
):
    acc[...] = acc_in[...]
    top[...] = top_in[...]
    tot[...] = tot_in[...]
    stat[...] = jnp.zeros_like(stat)
    for h in range(2):
        for i, part in enumerate(three_parts(jnp.full((1, TOK), lam_ref[h], F32))):
            stat[12 + 3 * h + i : 13 + 3 * h + i, :] = part

    def sending(o):
        home = (x_ref[0] + 4 - o) % 4
        return pltpu.make_async_copy(buf.at[o], out_ref.at[pl.ds(4 * home, 4)], sem.at[o])

    def block_done(o):
        for hm in range(4):
            total = tot[o, hm]
            mean = (acc[o, hm] / total).T.astype(BF16)
            buf[o, :, :, hm * VD : (hm + 1) * VD] = mean.reshape(4, TOK // 4, VD)
            for i, part in enumerate(three_parts(top[o, hm] + jnp.log2(total))):
                stat[3 * hm + i : 3 * hm + i + 1, :] = part
        buf[o, :, :, 4 * VD :] = stat[...].T.astype(BF16).reshape(4, TOK // 4, VD)
        sending(o).start()

    absorb(chunks_of(kv_ref), qs, sc, acc, top, tot, False, block_done)
    for o in range(4):
        sending(o).wait()


def cost(keys):
    return pl.CostEstimate(
        flops=2 * keys * 4 * TOK * 4 * 3 * HEAD,
        bytes_accessed=keys * 1024,
        transcendentals=keys * 4 * TOK * 4,
    )


def score_scratch(chunks):
    return pltpu.VMEM((2, chunks * TOK, TOK), F32)


def attend_first(queries, own, other):
    return pl.pallas_call(
        first_kernel,
        out_shape=(QS,) + STATE,
        in_specs=[VMEM] * 6,
        out_specs=(VMEM,) * 4,
        scratch_shapes=[score_scratch(2)],
        cost_estimate=cost(512),
        compiler_params=pltpu.CompilerParams(vmem_limit_bytes=24 * 2**20),
        name="attend_first",
    )(*queries, own, other)


def attend_next(qs, kv, state):
    keys = kv.shape[0] * TOK if len(kv.shape) == 3 else kv.shape[0] // 2
    return pl.pallas_call(
        next_kernel,
        out_shape=STATE,
        in_specs=[VMEM] * 5,
        out_specs=(VMEM,) * 3,
        input_output_aliases={2: 0, 3: 1, 4: 2},
        scratch_shapes=[score_scratch(keys // TOK)],
        cost_estimate=cost(keys),
        compiler_params=pltpu.CompilerParams(vmem_limit_bytes=24 * 2**20),
        name="attend_next",
    )(qs, kv, *state)


def attend_last(x, lambdas, qs, kv, state):
    return pl.pallas_call(
        last_kernel,
        out_shape=jax.ShapeDtypeStruct((16, TOK // 4, WIDE), BF16),
        in_specs=[SMEM, SMEM] + [VMEM] * 5,
        out_specs=HBM,
        scratch_shapes=[pltpu.VMEM(s.shape, s.dtype) for s in STATE]
        + [
            score_scratch(kv.shape[0] // (2 * TOK)),
            pltpu.VMEM((VD, TOK), F32),
            pltpu.VMEM((4, 4, TOK // 4, WIDE), BF16),
            pltpu.SemaphoreType.DMA((4,)),
        ],
        cost_estimate=cost(kv.shape[0] // 2),
        compiler_params=pltpu.CompilerParams(vmem_limit_bytes=24 * 2**20),
        name="attend_last",
    )(x, lambdas, qs, kv, *state)


def load_mix_kernel(w_ref, out_ref, sem):
    cuts = 4
    per = w_ref.shape[0] // cuts
    copies = []
    for i in range(cuts):
        rows = pl.ds(i * per, per)
        copies.append(pltpu.make_async_copy(w_ref.at[rows], out_ref.at[rows], sem.at[i]))
        copies[-1].start()
    for copy in copies:
        copy.wait()


def load_mix(weights):
    return pl.pallas_call(
        load_mix_kernel,
        out_shape=jax.ShapeDtypeStruct(weights.shape, BF16),
        in_specs=[HBM],
        out_specs=VMEM,
        scratch_shapes=[pltpu.SemaphoreType.DMA((4,))],
        compiler_params=pltpu.CompilerParams(vmem_limit_bytes=20 * 2**20),
        name="load_mix",
    )(weights)


def merge_kernel(
    at_ref, part_ref, gain_ref, res_ref, norm_ref, own_ref, mine_ref, other_ref, out_ref, wbuf, sem
):
    mine = at_ref[1] * VD
    copies = [[pltpu.make_async_copy(own_ref, wbuf.at[0], sem.at[0])]]
    for o in range(3):
        near, far = pl.ds(mine, VD), pl.ds(VD - mine, VD)
        copies.append(
            [
                pltpu.make_async_copy(mine_ref.at[o], wbuf.at[o + 1, near], sem.at[2 * o + 1]),
                pltpu.make_async_copy(other_ref.at[o], wbuf.at[o + 1, far], sem.at[2 * o + 2]),
            ]
        )
    for pair in copies:
        for copy in pair:
            copy.start()
    stream = res_ref[...].astype(F32)
    for o in range(4):
        y = (at_ref[0] + 4 - o) % 4
        parts = [part_ref[4 * k + y] for k in range(4)]
        stats = [p[:, 4 * VD :].astype(F32) for p in parts]
        heads = []
        for h in range(2):
            maps = []
            for m in range(2):
                hm = 2 * h + m
                at = 3 * hm
                lse = [s[:, at : at + 1] + s[:, at + 1 : at + 2] + s[:, at + 2 : at + 3] for s in stats]
                peak = jnp.maximum(jnp.maximum(lse[0], lse[1]), jnp.maximum(lse[2], lse[3]))
                share = [jnp.exp2(e - peak) for e in lse]
                inv = 1.0 / (share[0] + share[1] + share[2] + share[3])
                maps.append(
                    sum(
                        p[:, hm * VD : (hm + 1) * VD].astype(F32) * (w * inv)
                        for p, w in zip(parts, share)
                    )
                )
            at = 12 + 3 * h
            lam = stats[0][:, at : at + 1] + stats[0][:, at + 1 : at + 2] + stats[0][:, at + 2 : at + 3]
            diff = maps[0] - lam * maps[1]
            scale = lax.rsqrt(jnp.mean(diff * diff, axis=-1, keepdims=True) + 1e-05)
            heads.append((diff * scale * gain_ref[...] * 0.8).astype(BF16))
        flat = jnp.concatenate(heads, axis=1)
        for copy in copies[o]:
            copy.wait()
        stream = stream + lax.dot_general(flat, wbuf[o], NN, preferred_element_type=F32)
    center = stream - jnp.mean(stream, axis=-1, keepdims=True)
    spread = jnp.mean(center * center, axis=-1, keepdims=True)
    out_ref[...] = (center * lax.rsqrt(spread + 1e-05) * norm_ref[...]).astype(BF16)


def merge(at, part, head_gain, residual, norm_gain, weights):
    rows, width = residual.shape
    return pl.pallas_call(
        merge_kernel,
        out_shape=jax.ShapeDtypeStruct((rows, width), BF16),
        in_specs=[SMEM] + [VMEM] * 4 + [HBM] * 3,
        out_specs=VMEM,
        scratch_shapes=[pltpu.VMEM((4, 2 * VD, width), BF16), pltpu.SemaphoreType.DMA((7,))],
        compiler_params=pltpu.CompilerParams(vmem_limit_bytes=24 * 2**20),
        name="merge",
    )(at, part, head_gain.reshape(1, VD), residual, norm_gain.reshape(1, width), *weights)


def mixer_kernel(count, *refs):
    pieces, w_ref, outs = refs[:count], refs[count], refs[count + 1 :]
    devices, _, rows, hidden_width = w_ref.shape
    x = jnp.concatenate([n[...] for n in pieces], axis=0)
    cuts = 4
    per = devices // cuts
    step = per * rows
    lifted = None
    for i in range(cuts):
        block = w_ref[i * per : (i + 1) * per, 0].reshape(step, hidden_width)
        more = lax.dot_general(x[:, i * step : (i + 1) * step], block, NN, preferred_element_type=F32)
        lifted = more if lifted is None else lifted + more
    pos = jnp.maximum(lifted, 0.0)
    hidden = (pos * pos).astype(BF16)
    for i in range(cuts):
        block = w_ref[i * per : (i + 1) * per, 1].reshape(step, hidden_width)
        low = lax.dot_general(hidden, block, NT, preferred_element_type=F32)
        at = 0
        for n, o in zip(pieces, outs):
            o[:, i * step : (i + 1) * step] = low[at : at + o.shape[0]].astype(o.dtype)
            at += o.shape[0]


def mixer(pieces, weights, types):
    width = pieces[0].shape[1]
    return pl.pallas_call(
        functools.partial(mixer_kernel, len(pieces)),
        out_shape=[jax.ShapeDtypeStruct(n.shape, t) for n, t in zip(pieces, types)],
        in_specs=[VMEM] * (len(pieces) + 1),
        out_specs=[VMEM] * len(pieces),
        cost_estimate=pl.CostEstimate(flops=2 * 256 * width * 2048, bytes_accessed=2**23, transcendentals=0),
        compiler_params=pltpu.CompilerParams(vmem_limit_bytes=24 * 2**20),
        name="mixer",
    )(*pieces, weights)


def shifted(value, axis, by):
    size = lax.axis_size(axis)
    return lax.ppermute(value, axis, [(i, (i + by) % size) for i in range(size)])


def local(
    residual,
    first_query,
    second_query,
    first_key,
    second_key,
    values,
    lambdas,
    head_gain,
    out_weight,
    norm_gain,
    up_weight,
    down_weight,
):
    sp = lax.axis_index(("z", "x", "c"))
    x = lax.axis_index("x").astype(jnp.int32).reshape(1)
    at = jnp.stack([lax.axis_index("tp"), lax.axis_index("c")]).astype(jnp.int32)
    query, kv, query_own, kv_own = prepare(first_query, second_query, first_key, second_key, values, sp * TOK)
    ring = ("z", "c")
    onward = [(2 * z + c, 2 * ((z + 1 - 2 * c) % 8) + c) for z in range(8) for c in range(2)]
    crossed = [(2 * z + c, 2 * ((z - 1 + 2 * c) % 8) + 1 - c) for z in range(8) for c in range(2)]
    near = [lax.ppermute(kv, ring, onward), lax.ppermute(kv, ring, crossed)]
    other = shifted(kv, "c", 1)
    queries = [query_own] + [shifted(query, "x", o) for o in (1, 2, 3)]
    mix_weights = jnp.stack([up_weight, down_weight.T])
    mix_weights = lax.all_gather(mix_weights, ("z", "x", "c"))
    half = lax.dynamic_slice_in_dim(out_weight, lax.axis_index("c") * VD, VD, 0)
    near = jnp.stack(near)
    second = lax.ppermute(near, ring, onward)
    mine = jnp.stack([shifted(half, "tp", o) for o in (1, 2, 3)])
    out_weights = [out_weight, mine, shifted(mine, "c", 1)]
    qs, *state = attend_first(queries, kv_own, other)
    third = lax.ppermute(second, ring, onward)
    four = jnp.concatenate([near, second])
    four_other = shifted(four, "c", 1)
    state = attend_next(qs, four, state)
    state = attend_next(qs, four_other, state)
    far = lax.ppermute(third[0], ring, onward)
    third_other = shifted(third, "c", 1)
    state = attend_next(qs, third, state)
    state = attend_next(qs, third_other, state)
    far_other = shifted(far, "c", 1)
    state = attend_next(qs, far, state)
    part = attend_last(x, lambdas, qs, far_other, state)
    part = lax.all_to_all(part, ("x", "tp"), split_axis=0, concat_axis=0, tiled=True)
    normed = merge(at, part, head_gain, residual, norm_gain, out_weights)
    mix_weights = load_mix(mix_weights)
    rows = normed.shape[0] // 2
    before = shifted(normed, "tp", 1)
    after = shifted(normed, "tp", -1)
    cut1 = before[:rows]
    cut3 = after[rows:]
    across1 = shifted(cut1, "tp", 1)
    across3 = shifted(cut3, "tp", -1)
    low0, low1, low3 = mixer([normed, before, after], mix_weights, (F32, BF16, BF16))
    low1 = shifted(low1, "tp", -1)
    low3 = shifted(low3, "tp", 1)
    across = jnp.concatenate([across1, across3])
    (low2,) = mixer([across], mix_weights, (BF16,))
    low2 = shifted(low2, "tp", 2)
    total = normed.astype(F32) + low0
    for low in (low1, low2, low3):
        total = total + low.astype(F32)
    return total.astype(BF16)


def solution(mesh):
    fine = Mesh(mesh.devices.reshape(8, 4, 2, 4), ("z", "x", "c", "tp"))
    sp = ("z", "x", "c")
    in_specs = (
        P(sp + ("tp",), None),
        P(sp, "tp"),
        P(sp, "tp"),
        P(sp, "tp"),
        P(sp, "tp"),
        P(sp, "tp"),
        P("tp"),
        P(),
        P("tp", None),
        P(),
        P(sp, "tp"),
        P("tp", sp),
    )
    out_specs = P(sp + ("tp",), None)

    return jax.shard_map(local, mesh=fine, in_specs=in_specs, out_specs=out_specs, check_vma=False)
```

```python
import functools

import jax
import jax.numpy as jnp
from jax import lax
from jax.experimental import pallas as pl
from jax.experimental.pallas import tpu as pltpu
from jax.sharding import Mesh, PartitionSpec as P


F32 = jnp.float32
BF16 = jnp.bfloat16
TOK = 256
HEAD = 64
VD = 128
LOG2E = 1.4426950408889634
NT = (((1,), (1,)), ((), ()))
NN = (((1,), (0,)), ((), ()))
HBM = pl.BlockSpec(memory_space=pltpu.HBM)
SMEM = pl.BlockSpec(memory_space=pltpu.SMEM)
VMEM = pl.BlockSpec(memory_space=pltpu.VMEM)


def prep_kernel(cos_ref, sin_ref, qa_ref, qb_ref, ka_ref, kb_ref, v_ref, q_out, kv_out, q_own, kv_own):
    cos = jnp.concatenate([cos_ref[...]] * 4, axis=1)
    sin = jnp.concatenate([-sin_ref[...], sin_ref[...]] * 2, axis=1)
    lane = lax.broadcasted_iota(jnp.int32, cos.shape, 1)
    front = (lane % HEAD) < HEAD // 2

    def turn(ref):
        x = ref[...].astype(F32)
        other = jnp.where(front, pltpu.roll(x, 128 - 32, 1), pltpu.roll(x, 32, 1))
        return (x * cos + other * sin).astype(BF16)

    q_out[:, 0:128] = turn(qa_ref)
    q_out[:, 128:256] = turn(qb_ref)
    kv_out[0:TOK, 0:128] = turn(ka_ref)
    kv_out[0:TOK, 128:256] = turn(kb_ref)
    kv_out[TOK : 2 * TOK, :] = v_ref[...].astype(F32).T.astype(BF16)
    q_own[...] = q_out[...]
    kv_own[...] = kv_out[...]


def prepare(first_query, second_query, first_key, second_key, values, start):
    positions = (start + jnp.arange(TOK)).astype(F32)
    half = HEAD // 2
    inverse = 10000.0 ** (-jnp.arange(0, half, dtype=F32) * 2.0 / HEAD)
    angle = positions[:, None] * inverse[None, :]
    cos, sin = jnp.cos(angle), jnp.sin(angle)
    return pl.pallas_call(
        prep_kernel,
        out_shape=(
            jax.ShapeDtypeStruct((TOK, 2 * VD), BF16),
            jax.ShapeDtypeStruct((2 * TOK, 2 * VD), BF16),
        )
        * 2,
        in_specs=[VMEM] * 7,
        out_specs=(VMEM,) * 4,
        name="prep",
    )(cos, sin, first_query, second_query, first_key, second_key, values)


def load_queries(queries, qs):
    lane = lax.broadcasted_iota(jnp.int32, (TOK, 128), 1)
    for o, q in enumerate(queries):
        for m in range(2):
            scaled = q[:, m * 128 : (m + 1) * 128].astype(F32) * (LOG2E * HEAD**-0.5)
            hi = scaled.astype(BF16).astype(F32)
            lo = scaled - hi
            for h in range(2):
                mine = (lane < HEAD) if h == 0 else (lane >= HEAD)
                qs[o, 2 * h + m, :, 0:128] = jnp.where(mine, hi, 0.0).astype(BF16)
                qs[o, 2 * h + m, :, 128:256] = jnp.where(mine, lo, 0.0).astype(BF16)


def absorb(chunks, qs, sc, acc, top, tot, fresh):
    def scores(slot, o, hm):
        m = hm % 2
        keys = jnp.concatenate([c[0:TOK, m * 128 : (m + 1) * 128] for c in chunks], axis=0)
        both = jnp.concatenate([keys, keys], axis=1)
        s = lax.dot_general(both, qs[o, hm], NT, preferred_element_type=F32)
        sc[slot] = s
        return jnp.max(s, axis=0, keepdims=True)

    def step(o, peak):
        after = jnp.minimum(o + 1, 3)
        for hm in range(4):
            here = peak
            peak = scores((hm + 1) % 2, o, hm + 1) if hm < 3 else scores(0, after, 0)
            h = hm // 2
            if fresh:
                new = here
            else:
                old = top[o, hm]
                new = jnp.maximum(old, here)
                shrink = jnp.exp2(old - new)
            p = jnp.exp2(sc[hm % 2] - new)
            vals = jnp.concatenate([c[TOK + h * VD : TOK + (h + 1) * VD, :] for c in chunks], axis=1)
            moved = lax.dot_general(vals, p.astype(BF16), NN, preferred_element_type=F32)
            total = jnp.sum(p, axis=0, keepdims=True)
            top[o, hm] = new
            if fresh:
                tot[o, hm] = total
                acc[o, hm] = moved
            else:
                tot[o, hm] = tot[o, hm] * shrink + total
                acc[o, hm] = acc[o, hm] * shrink + moved
        return peak

    lax.fori_loop(0, 4, step, scores(0, 0, 0))


STATE = (
    jax.ShapeDtypeStruct((4, 4, VD, TOK), F32),
    jax.ShapeDtypeStruct((4, 4, 1, TOK), F32),
    jax.ShapeDtypeStruct((4, 4, 1, TOK), F32),
)
QS = jax.ShapeDtypeStruct((4, 4, TOK, 2 * VD), BF16)


def chunks_of(ref):
    return [ref] if len(ref.shape) == 2 else [ref.at[i] for i in range(ref.shape[0])]


def first_kernel(q0, q1, q2, q3, own_ref, other_ref, qs, acc, top, tot, sc):
    load_queries((q0, q1, q2, q3), qs)
    absorb([own_ref, other_ref], qs, sc, acc, top, tot, True)


def next_kernel(qs, kv_ref, acc_in, top_in, tot_in, acc, top, tot, sc):
    absorb(chunks_of(kv_ref), qs, sc, acc, top, tot, False)


def last_kernel(qs, kv_ref, acc_in, top_in, tot_in, acc, top, tot, lse, sc):
    absorb(chunks_of(kv_ref), qs, sc, acc, top, tot, False)
    for o in range(4):
        for hm in range(4):
            row = 4 * o + hm
            lse[row : row + 1, :] = top[o, hm] + jnp.log2(tot[o, hm])


def share_kernel(x_ref, lam_ref, lse0, lse1, lse2, lse3, acc, tot, out_ref):
    lses = (lse0, lse1, lse2, lse3)
    for o in range(4):
        home = (x_ref[0] + 4 - o) % 4
        factors = []
        for hm in range(4):
            rows = [4 * ((o - k) % 4) + hm for k in range(4)]
            here = [ref[row : row + 1, :] for ref, row in zip(lses, rows)]
            peak = jnp.maximum(jnp.maximum(here[0], here[1]), jnp.maximum(here[2], here[3]))
            terms = [jnp.exp2(e - peak) for e in here]
            factors.append(terms[0] / ((terms[0] + terms[1] + terms[2] + terms[3]) * tot[o, hm]))
        for h in range(2):
            diff = acc[o, 2 * h] * factors[2 * h] - acc[o, 2 * h + 1] * (lam_ref[h] * factors[2 * h + 1])
            out_ref[pl.ds(4 * home, 4), :, h * VD : (h + 1) * VD] = diff.T.astype(BF16).reshape(
                4, TOK // 4, VD
            )


def cost(keys):
    return pl.CostEstimate(
        flops=2 * keys * 4 * TOK * 4 * 3 * HEAD,
        bytes_accessed=keys * 1024,
        transcendentals=keys * 4 * TOK * 4,
    )


def score_scratch(chunks):
    return pltpu.VMEM((2, chunks * TOK, TOK), F32)


def attend_first(queries, own, other):
    return pl.pallas_call(
        first_kernel,
        out_shape=(QS,) + STATE,
        in_specs=[VMEM] * 6,
        out_specs=(VMEM,) * 4,
        scratch_shapes=[score_scratch(2)],
        cost_estimate=cost(512),
        compiler_params=pltpu.CompilerParams(vmem_limit_bytes=24 * 2**20),
        name="attend_first",
    )(*queries, own, other)


def attend_next(qs, kv, state):
    keys = kv.shape[0] * TOK if len(kv.shape) == 3 else kv.shape[0] // 2
    return pl.pallas_call(
        next_kernel,
        out_shape=STATE,
        in_specs=[VMEM] * 5,
        out_specs=(VMEM,) * 3,
        input_output_aliases={2: 0, 3: 1, 4: 2},
        scratch_shapes=[score_scratch(keys // TOK)],
        cost_estimate=cost(keys),
        compiler_params=pltpu.CompilerParams(vmem_limit_bytes=24 * 2**20),
        name="attend_next",
    )(qs, kv, *state)


def attend_last(qs, kv, state):
    return pl.pallas_call(
        last_kernel,
        out_shape=STATE + (jax.ShapeDtypeStruct((16, TOK), F32),),
        in_specs=[VMEM] * 5,
        out_specs=(VMEM,) * 4,
        input_output_aliases={2: 0, 3: 1, 4: 2},
        scratch_shapes=[score_scratch(kv.shape[0] // (2 * TOK))],
        cost_estimate=cost(kv.shape[0] // 2),
        compiler_params=pltpu.CompilerParams(vmem_limit_bytes=24 * 2**20),
        name="attend_last",
    )(qs, kv, *state)


def share(x, lambdas, lses, acc, tot):
    return pl.pallas_call(
        share_kernel,
        out_shape=jax.ShapeDtypeStruct((16, TOK // 4, 2 * VD), BF16),
        in_specs=[SMEM, SMEM] + [VMEM] * 6,
        out_specs=VMEM,
        compiler_params=pltpu.CompilerParams(vmem_limit_bytes=16 * 2**20),
        name="share",
    )(x, lambdas, *lses, acc, tot)


def load_mix_kernel(w_ref, out_ref, sem):
    cuts = 4
    per = w_ref.shape[0] // cuts
    copies = []
    for i in range(cuts):
        rows = pl.ds(i * per, per)
        copies.append(pltpu.make_async_copy(w_ref.at[rows], out_ref.at[rows], sem.at[i]))
        copies[-1].start()
    for copy in copies:
        copy.wait()


def load_mix(weights):
    return pl.pallas_call(
        load_mix_kernel,
        out_shape=jax.ShapeDtypeStruct(weights.shape, BF16),
        in_specs=[HBM],
        out_specs=VMEM,
        scratch_shapes=[pltpu.SemaphoreType.DMA((4,))],
        compiler_params=pltpu.CompilerParams(vmem_limit_bytes=20 * 2**20),
        name="load_mix",
    )(weights)


def merge_kernel(at_ref, part_ref, gain_ref, res_ref, norm_ref, mine_ref, other_ref, out_ref, wbuf, sem):
    mine = at_ref[1] * VD
    copies = []
    for o in range(4):
        near, far = pl.ds(mine, VD), pl.ds(VD - mine, VD)
        copies.append(
            [
                pltpu.make_async_copy(mine_ref.at[o], wbuf.at[o, near], sem.at[2 * o]),
                pltpu.make_async_copy(other_ref.at[o], wbuf.at[o, far], sem.at[2 * o + 1]),
            ]
        )
    for pair in copies:
        for copy in pair:
            copy.start()
    stream = res_ref[...].astype(F32)
    for o in range(4):
        y = (at_ref[0] + 4 - o) % 4
        both = sum(part_ref[4 * k + y].astype(F32) for k in range(4))
        heads = []
        for h in range(2):
            diff = both[:, h * VD : (h + 1) * VD]
            scale = lax.rsqrt(jnp.mean(diff * diff, axis=-1, keepdims=True) + 1e-05)
            heads.append((diff * scale * gain_ref[...] * 0.8).astype(BF16))
        flat = jnp.concatenate(heads, axis=1)
        for copy in copies[o]:
            copy.wait()
        stream = stream + lax.dot_general(flat, wbuf[o], NN, preferred_element_type=F32)
    center = stream - jnp.mean(stream, axis=-1, keepdims=True)
    spread = jnp.mean(center * center, axis=-1, keepdims=True)
    out_ref[...] = (center * lax.rsqrt(spread + 1e-05) * norm_ref[...]).astype(BF16)


def merge(at, part, head_gain, residual, norm_gain, weights):
    rows, width = residual.shape
    return pl.pallas_call(
        merge_kernel,
        out_shape=jax.ShapeDtypeStruct((rows, width), BF16),
        in_specs=[SMEM] + [VMEM] * 4 + [HBM] * 2,
        out_specs=VMEM,
        scratch_shapes=[pltpu.VMEM((4, 2 * VD, width), BF16), pltpu.SemaphoreType.DMA((8,))],
        compiler_params=pltpu.CompilerParams(vmem_limit_bytes=24 * 2**20),
        name="merge",
    )(at, part, head_gain.reshape(1, VD), residual, norm_gain.reshape(1, width), *weights)


def mixer_kernel(count, *refs):
    pieces, w_ref, outs = refs[:count], refs[count], refs[count + 1 :]
    devices, _, rows, hidden_width = w_ref.shape
    x = jnp.concatenate([n[...] for n in pieces], axis=0)
    cuts = 4
    per = devices // cuts
    step = per * rows
    lifted = None
    for i in range(cuts):
        block = w_ref[i * per : (i + 1) * per, 0].reshape(step, hidden_width)
        more = lax.dot_general(x[:, i * step : (i + 1) * step], block, NN, preferred_element_type=F32)
        lifted = more if lifted is None else lifted + more
    pos = jnp.maximum(lifted, 0.0)
    hidden = (pos * pos).astype(BF16)
    for i in range(cuts):
        block = w_ref[i * per : (i + 1) * per, 1].reshape(step, hidden_width)
        low = lax.dot_general(hidden, block, NT, preferred_element_type=F32)
        at = 0
        for n, o in zip(pieces, outs):
            o[:, i * step : (i + 1) * step] = low[at : at + o.shape[0]].astype(o.dtype)
            at += o.shape[0]


def mixer(pieces, weights, types):
    width = pieces[0].shape[1]
    return pl.pallas_call(
        functools.partial(mixer_kernel, len(pieces)),
        out_shape=[jax.ShapeDtypeStruct(n.shape, t) for n, t in zip(pieces, types)],
        in_specs=[VMEM] * (len(pieces) + 1),
        out_specs=[VMEM] * len(pieces),
        cost_estimate=pl.CostEstimate(flops=2 * 256 * width * 2048, bytes_accessed=2**23, transcendentals=0),
        compiler_params=pltpu.CompilerParams(vmem_limit_bytes=24 * 2**20),
        name="mixer",
    )(*pieces, weights)


def shifted(value, axis, by):
    size = lax.axis_size(axis)
    return lax.ppermute(value, axis, [(i, (i + by) % size) for i in range(size)])


def local(
    residual,
    first_query,
    second_query,
    first_key,
    second_key,
    values,
    lambdas,
    head_gain,
    out_weight,
    norm_gain,
    up_weight,
    down_weight,
):
    sp = lax.axis_index(("z", "x", "c"))
    x = lax.axis_index("x").astype(jnp.int32).reshape(1)
    at = jnp.stack([lax.axis_index("tp"), lax.axis_index("c")]).astype(jnp.int32)
    query, kv, query_own, kv_own = prepare(first_query, second_query, first_key, second_key, values, sp * TOK)
    ring = ("z", "c")
    onward = [(2 * z + c, 2 * ((z + 1 - 2 * c) % 8) + c) for z in range(8) for c in range(2)]
    crossed = [(2 * z + c, 2 * ((z - 1 + 2 * c) % 8) + 1 - c) for z in range(8) for c in range(2)]
    near = [lax.ppermute(kv, ring, onward), lax.ppermute(kv, ring, crossed)]
    other = shifted(kv, "c", 1)
    queries = [query_own] + [shifted(query, "x", o) for o in (1, 2, 3)]
    mix_weights = jnp.stack([up_weight, down_weight.T])
    mix_weights = lax.all_gather(mix_weights, ("z", "x", "c"))
    half = lax.dynamic_slice_in_dim(out_weight, lax.axis_index("c") * VD, VD, 0)
    near = jnp.stack(near)
    second = lax.ppermute(near, ring, onward)
    mine = jnp.stack([half] + [shifted(half, "tp", o) for o in (1, 2, 3)])
    out_weights = [mine, shifted(mine, "c", 1)]
    qs, *state = attend_first(queries, kv_own, other)
    third = lax.ppermute(second, ring, onward)
    four = jnp.concatenate([near, second])
    four_other = shifted(four, "c", 1)
    state = attend_next(qs, four, state)
    state = attend_next(qs, four_other, state)
    far = lax.ppermute(third[0], ring, onward)
    third_other = shifted(third, "c", 1)
    state = attend_next(qs, third, state)
    state = attend_next(qs, third_other, state)
    far_other = shifted(far, "c", 1)
    *state, _ = attend_last(qs, far, state)
    acc, _, tot, lse = attend_last(qs, far_other, state)
    lses = [lse] + [shifted(lse, "x", k) for k in (1, 2, 3)]
    part = share(x, lambdas, lses, acc, tot)
    part = lax.all_to_all(part, ("x", "tp"), split_axis=0, concat_axis=0, tiled=True)
    normed = merge(at, part, head_gain, residual, norm_gain, out_weights)
    mix_weights = load_mix(mix_weights)
    rows = normed.shape[0] // 2
    before = shifted(normed, "tp", 1)
    after = shifted(normed, "tp", -1)
    cut1 = before[:rows]
    cut3 = after[rows:]
    across1 = shifted(cut1, "tp", 1)
    across3 = shifted(cut3, "tp", -1)
    low0, low1, low3 = mixer([normed, before, after], mix_weights, (F32, BF16, BF16))
    low1 = shifted(low1, "tp", -1)
    low3 = shifted(low3, "tp", 1)
    across = jnp.concatenate([across1, across3])
    (low2,) = mixer([across], mix_weights, (BF16,))
    low2 = shifted(low2, "tp", 2)
    total = normed.astype(F32) + low0
    for low in (low1, low2, low3):
        total = total + low.astype(F32)
    return total.astype(BF16)


def solution(mesh):
    fine = Mesh(mesh.devices.reshape(8, 4, 2, 4), ("z", "x", "c", "tp"))
    sp = ("z", "x", "c")
    in_specs = (
        P(sp + ("tp",), None),
        P(sp, "tp"),
        P(sp, "tp"),
        P(sp, "tp"),
        P(sp, "tp"),
        P(sp, "tp"),
        P("tp"),
        P(),
        P("tp", None),
        P(),
        P(sp, "tp"),
        P("tp", sp),
    )
    out_specs = P(sp + ("tp",), None)

    return jax.shard_map(local, mesh=fine, in_specs=in_specs, out_specs=out_specs, check_vma=False)
```

```python
import functools

import jax
import jax.numpy as jnp
from jax import lax
from jax.experimental import pallas as pl
from jax.experimental.pallas import tpu as pltpu
from jax.sharding import Mesh, PartitionSpec as P


F32 = jnp.float32
BF16 = jnp.bfloat16
TOK = 256
HEAD = 64
VD = 128
LOG2E = 1.4426950408889634
NT = (((1,), (1,)), ((), ()))
NN = (((1,), (0,)), ((), ()))
HBM = pl.BlockSpec(memory_space=pltpu.HBM)
SMEM = pl.BlockSpec(memory_space=pltpu.SMEM)
VMEM = pl.BlockSpec(memory_space=pltpu.VMEM)


def prep_kernel(
    cos_ref, sin_ref, qa_ref, qb_ref, ka_ref, kb_ref, v_ref, up_ref, down_ref,
    q_out, kv_out, q_own, kv_own, mix_out, sem,
):
    copies = [
        pltpu.make_async_copy(ref, mix_out.at[i], sem.at[i]) for i, ref in enumerate((up_ref, down_ref))
    ]
    for copy in copies:
        copy.start()
    rows = TOK // 4
    lane = lax.broadcasted_iota(jnp.int32, (rows, 128), 1)
    front = (lane % HEAD) < HEAD // 2

    def turn_rows(i, carry):
        at = pl.ds(pl.multiple_of(i * rows, rows), rows)
        cos = jnp.concatenate([cos_ref[at, :]] * 4, axis=1)
        sin = jnp.concatenate([-sin_ref[at, :], sin_ref[at, :]] * 2, axis=1)

        def turn(ref):
            x = ref[at, :].astype(F32)
            other = jnp.where(front, pltpu.roll(x, 128 - 32, 1), pltpu.roll(x, 32, 1))
            return (x * cos + other * sin).astype(BF16)

        q_out[at, 0:128] = turn(qa_ref)
        q_out[at, 128:256] = turn(qb_ref)
        kv_out[at, 0:128] = turn(ka_ref)
        kv_out[at, 128:256] = turn(kb_ref)
        return carry

    lax.fori_loop(0, 4, turn_rows, 0)
    kv_out[TOK : 2 * TOK, :] = v_ref[...].astype(F32).T.astype(BF16)
    q_own[...] = q_out[...]
    kv_own[...] = kv_out[...]
    for copy in copies:
        copy.wait()


def prepare(first_query, second_query, first_key, second_key, values, up, down, start):
    positions = (start + jnp.arange(TOK)).astype(F32)
    half = HEAD // 2
    inverse = 10000.0 ** (-jnp.arange(0, half, dtype=F32) * 2.0 / HEAD)
    angle = positions[:, None] * inverse[None, :]
    cos, sin = jnp.cos(angle), jnp.sin(angle)
    return pl.pallas_call(
        prep_kernel,
        out_shape=(
            jax.ShapeDtypeStruct((TOK, 2 * VD), BF16),
            jax.ShapeDtypeStruct((2 * TOK, 2 * VD), BF16),
        )
        * 2
        + (jax.ShapeDtypeStruct((2,) + up.shape, BF16),),
        in_specs=[VMEM] * 7 + [HBM] * 2,
        out_specs=(VMEM,) * 4 + (HBM,),
        scratch_shapes=[pltpu.SemaphoreType.DMA((2,))],
        name="prep",
    )(cos, sin, first_query, second_query, first_key, second_key, values, up, down)


def load_queries(queries, qs):
    rows = TOK // 4
    lane = lax.broadcasted_iota(jnp.int32, (rows, 128), 1)

    def load(i, carry):
        at = pl.ds(pl.multiple_of(i * rows, rows), rows)
        for o, q in enumerate(queries):
            for m in range(2):
                scaled = q[at, m * 128 : (m + 1) * 128].astype(F32) * (LOG2E * HEAD**-0.5)
                hi = scaled.astype(BF16).astype(F32)
                lo = scaled - hi
                for h in range(2):
                    mine = (lane < HEAD) if h == 0 else (lane >= HEAD)
                    qs[o, 2 * h + m, at, 0:128] = jnp.where(mine, hi, 0.0).astype(BF16)
                    qs[o, 2 * h + m, at, 128:256] = jnp.where(mine, lo, 0.0).astype(BF16)
        return carry

    lax.fori_loop(0, 4, load, 0)


def absorb(chunks, qs, sc, acc, top, tot, fresh):
    def scores(slot, o, hm):
        m = hm % 2
        keys = jnp.concatenate([c[0:TOK, m * 128 : (m + 1) * 128] for c in chunks], axis=0)
        both = jnp.concatenate([keys, keys], axis=1)
        s = lax.dot_general(both, qs[o, hm], NT, preferred_element_type=F32)
        sc[slot] = s
        return jnp.max(s, axis=0, keepdims=True)

    def step(o, peak):
        after = jnp.minimum(o + 1, 3)
        for hm in range(4):
            here = peak
            peak = scores((hm + 1) % 2, o, hm + 1) if hm < 3 else scores(0, after, 0)
            h = hm // 2
            if fresh:
                new = here
            else:
                old = top[o, hm]
                new = jnp.maximum(old, here)
                shrink = jnp.exp2(old - new)
            p = jnp.exp2(sc[hm % 2] - new)
            vals = jnp.concatenate([c[TOK + h * VD : TOK + (h + 1) * VD, :] for c in chunks], axis=1)
            moved = lax.dot_general(vals, p.astype(BF16), NN, preferred_element_type=F32)
            total = jnp.sum(p, axis=0, keepdims=True)
            top[o, hm] = new
            if fresh:
                tot[o, hm] = total
                acc[o, hm] = moved
            else:
                tot[o, hm] = tot[o, hm] * shrink + total
                acc[o, hm] = acc[o, hm] * shrink + moved
        return peak

    lax.fori_loop(0, 4, step, scores(0, 0, 0))


STATE = (
    jax.ShapeDtypeStruct((4, 4, VD, TOK), F32),
    jax.ShapeDtypeStruct((4, 4, 1, TOK), F32),
    jax.ShapeDtypeStruct((4, 4, 1, TOK), F32),
)
QS = jax.ShapeDtypeStruct((4, 4, TOK, 2 * VD), BF16)


def chunks_of(ref):
    return [ref] if len(ref.shape) == 2 else [ref.at[i] for i in range(ref.shape[0])]


def first_kernel(q0, q1, q2, q3, own_ref, other_ref, qs, acc, top, tot, sc):
    load_queries((q0, q1, q2, q3), qs)
    absorb([own_ref, other_ref], qs, sc, acc, top, tot, True)


def next_kernel(qs, kv_ref, acc_in, top_in, tot_in, acc, top, tot, sc):
    absorb(chunks_of(kv_ref), qs, sc, acc, top, tot, False)


def last_kernel(qs, kv_ref, acc_in, top_in, tot_in, lse_in, acc, top, tot, lse, sc):
    absorb(chunks_of(kv_ref), qs, sc, acc, top, tot, False)
    for o in range(4):
        for hm in range(4):
            row = 4 * o + hm
            lse[row : row + 1, :] = top[o, hm] + jnp.log2(tot[o, hm])


def share_kernel(lam_ref, lse0, lse1, lse2, lse3, acc, tot, *outs):
    lses = (lse0, lse1, lse2, lse3)
    for o in range(4):
        factors = []
        for hm in range(4):
            rows = [4 * ((o - k) % 4) + hm for k in range(4)]
            here = [ref[row : row + 1, :] for ref, row in zip(lses, rows)]
            peak = jnp.maximum(jnp.maximum(here[0], here[1]), jnp.maximum(here[2], here[3]))
            terms = [jnp.exp2(e - peak) for e in here]
            factors.append(terms[0] / ((terms[0] + terms[1] + terms[2] + terms[3]) * tot[o, hm]))
        for h in range(2):
            diff = acc[o, 2 * h] * factors[2 * h] - acc[o, 2 * h + 1] * (lam_ref[h] * factors[2 * h + 1])
            outs[o][:, h * VD : (h + 1) * VD] = diff.T.astype(BF16)


def cost(keys):
    return pl.CostEstimate(
        flops=2 * keys * 4 * TOK * 4 * 3 * HEAD,
        bytes_accessed=keys * 1024,
        transcendentals=keys * 4 * TOK * 4,
    )


def score_scratch(chunks):
    return pltpu.VMEM((2, chunks * TOK, TOK), F32)


def attend_first(queries, own, other):
    return pl.pallas_call(
        first_kernel,
        out_shape=(QS,) + STATE,
        in_specs=[VMEM] * 6,
        out_specs=(VMEM,) * 4,
        scratch_shapes=[score_scratch(2)],
        cost_estimate=cost(512),
        compiler_params=pltpu.CompilerParams(vmem_limit_bytes=24 * 2**20),
        name="attend_first",
    )(*queries, own, other)


def attend_next(qs, kv, state):
    keys = kv.shape[0] * TOK if len(kv.shape) == 3 else kv.shape[0] // 2
    return pl.pallas_call(
        next_kernel,
        out_shape=STATE,
        in_specs=[VMEM] * 5,
        out_specs=(VMEM,) * 3,
        input_output_aliases={2: 0, 3: 1, 4: 2},
        scratch_shapes=[score_scratch(keys // TOK)],
        cost_estimate=cost(keys),
        compiler_params=pltpu.CompilerParams(vmem_limit_bytes=24 * 2**20),
        name="attend_next",
    )(qs, kv, *state)


def attend_last(qs, kv, state):
    return pl.pallas_call(
        last_kernel,
        out_shape=STATE + (jax.ShapeDtypeStruct((16, TOK), F32),),
        in_specs=[VMEM] * 6,
        out_specs=(VMEM,) * 4,
        input_output_aliases={2: 0, 3: 1, 4: 2, 5: 3},
        scratch_shapes=[score_scratch(kv.shape[0] // (2 * TOK))],
        cost_estimate=cost(kv.shape[0] // 2),
        compiler_params=pltpu.CompilerParams(vmem_limit_bytes=24 * 2**20),
        name="attend_last",
    )(qs, kv, *state)


def share(lambdas, lses, acc, tot):
    return pl.pallas_call(
        share_kernel,
        out_shape=[jax.ShapeDtypeStruct((TOK, 2 * VD), BF16)] * 4,
        in_specs=[SMEM] + [VMEM] * 6,
        out_specs=[VMEM] * 4,
        compiler_params=pltpu.CompilerParams(vmem_limit_bytes=16 * 2**20),
        name="share",
    )(lambdas, *lses, acc, tot)


def heads_kernel(at_ref, gain_ref, p0, p1, p2, p3, *refs):
    outs, buf = refs[:4], refs[4]
    whole = sum(p[...].astype(F32) for p in (p0, p1, p2, p3))
    for h in range(2):
        diff = whole[:, h * VD : (h + 1) * VD]
        scale = lax.rsqrt(jnp.mean(diff * diff, axis=-1, keepdims=True) + 1e-05)
        buf[:, h * VD : (h + 1) * VD] = (diff * scale * gain_ref[...] * 0.8).astype(BF16)
    for o in range(4):
        y = (at_ref[0] + o) % 4
        outs[o][...] = buf[pl.ds(y * (TOK // 4), TOK // 4), :]


def heads(at, head_gain, parts):
    return pl.pallas_call(
        heads_kernel,
        out_shape=[jax.ShapeDtypeStruct((TOK // 4, 2 * VD), BF16)] * 4,
        in_specs=[SMEM] + [VMEM] * 5,
        out_specs=[VMEM] * 4,
        scratch_shapes=[pltpu.VMEM((TOK, 2 * VD), BF16)],
        compiler_params=pltpu.CompilerParams(vmem_limit_bytes=12 * 2**20),
        name="heads",
    )(at, head_gain.reshape(1, VD), *parts)


def load_mix_kernel(w_ref, out_ref, sem):
    cuts = 4
    per = w_ref.shape[0] // cuts
    copies = []
    for i in range(cuts):
        rows = pl.ds(i * per, per)
        copies.append(pltpu.make_async_copy(w_ref.at[rows], out_ref.at[rows], sem.at[i]))
        copies[-1].start()
    for copy in copies:
        copy.wait()


def load_mix(weights):
    return pl.pallas_call(
        load_mix_kernel,
        out_shape=jax.ShapeDtypeStruct(weights.shape, BF16),
        in_specs=[HBM],
        out_specs=VMEM,
        scratch_shapes=[pltpu.SemaphoreType.DMA((4,))],
        compiler_params=pltpu.CompilerParams(vmem_limit_bytes=20 * 2**20),
        name="load_mix",
    )(weights)


def merge_kernel(at_ref, f0, f1, f2, f3, res_ref, norm_ref, mine_ref, other_ref, out_ref, wbuf, sums, sem):
    mine = at_ref[1] * VD
    copies = []
    for o in range(4):
        near, far = pl.ds(mine, VD), pl.ds(VD - mine, VD)
        copies.append(
            [
                pltpu.make_async_copy(mine_ref.at[o], wbuf.at[o, near], sem.at[2 * o]),
                pltpu.make_async_copy(other_ref.at[o], wbuf.at[o, far], sem.at[2 * o + 1]),
            ]
        )
    for pair in copies:
        for copy in pair:
            copy.start()
    flat = jnp.concatenate([f[...] for f in (f0, f1, f2, f3)], axis=1)
    for pair in copies:
        for copy in pair:
            copy.wait()
    width = out_ref.shape[1] // 8

    def project(i, carry):
        at = pl.ds(pl.multiple_of(i * width, 128), width)
        weight = wbuf[:, :, at].reshape(flat.shape[1], width)
        added = lax.dot_general(flat, weight, NN, preferred_element_type=F32)
        sums[:, at] = res_ref[:, at].astype(F32) + added
        return carry

    lax.fori_loop(0, 8, project, 0)
    stream = sums[...]
    center = stream - jnp.mean(stream, axis=-1, keepdims=True)
    spread = jnp.mean(center * center, axis=-1, keepdims=True)
    out_ref[...] = (center * lax.rsqrt(spread + 1e-05) * norm_ref[...]).astype(BF16)


def merge(at, flats, residual, norm_gain, weights):
    rows, width = residual.shape
    return pl.pallas_call(
        merge_kernel,
        out_shape=jax.ShapeDtypeStruct((rows, width), BF16),
        in_specs=[SMEM] + [VMEM] * 6 + [HBM] * 2,
        out_specs=VMEM,
        scratch_shapes=[pltpu.VMEM((4, 2 * VD, width), BF16), pltpu.VMEM((rows, width), F32), pltpu.SemaphoreType.DMA((8,))],
        compiler_params=pltpu.CompilerParams(vmem_limit_bytes=24 * 2**20),
        name="merge",
    )(at, *flats, residual, norm_gain.reshape(1, width), *weights)


CUTS = 4


def mixer_kernel(count, *refs):
    pieces, w_ref, outs = refs[:count], refs[count], refs[count + 1 : -2]
    lifted, hidden = refs[-2:]
    devices, _, rows, hidden_width = w_ref.shape
    per = devices // CUTS
    step = per * rows

    def lift(i, carry):
        at = pl.ds(pl.multiple_of(i * step, 128), step)
        x = jnp.concatenate([n[:, at] for n in pieces], axis=0)
        block = w_ref[pl.ds(i * per, per), 0].reshape(step, hidden_width)
        lifted[...] += lax.dot_general(x, block, NN, preferred_element_type=F32)
        return carry

    def lower(i, carry):
        at = pl.ds(pl.multiple_of(i * (step // 2), 128), step // 2)
        block = w_ref[pl.ds(i * (per // 2), per // 2), 1].reshape(step // 2, hidden_width)
        low = lax.dot_general(hidden[...], block, NT, preferred_element_type=F32)
        first = 0
        for o in outs:
            o[:, at] = low[first : first + o.shape[0]].astype(o.dtype)
            first += o.shape[0]
        return carry

    lifted[...] = jnp.zeros_like(lifted)
    lax.fori_loop(0, CUTS, lift, 0)
    pos = jnp.maximum(lifted[...], 0.0)
    hidden[...] = (pos * pos).astype(BF16)
    lax.fori_loop(0, 2 * CUTS, lower, 0)


def mixer(pieces, weights, types):
    width = pieces[0].shape[1]
    return pl.pallas_call(
        functools.partial(mixer_kernel, len(pieces)),
        out_shape=[jax.ShapeDtypeStruct(n.shape, t) for n, t in zip(pieces, types)],
        in_specs=[VMEM] * (len(pieces) + 1),
        out_specs=[VMEM] * len(pieces),
        scratch_shapes=[pltpu.VMEM((sum(n.shape[0] for n in pieces), weights.shape[3]), t) for t in (F32, BF16)],
        cost_estimate=pl.CostEstimate(flops=2 * 256 * width * 2048, bytes_accessed=2**23, transcendentals=0),
        compiler_params=pltpu.CompilerParams(vmem_limit_bytes=24 * 2**20),
        name="mixer",
    )(*pieces, weights)


def shifted(value, axis, by):
    size = lax.axis_size(axis)
    return lax.ppermute(value, axis, [(i, (i + by) % size) for i in range(size)])


def local(
    residual,
    first_query,
    second_query,
    first_key,
    second_key,
    values,
    lambdas,
    head_gain,
    out_weight,
    norm_gain,
    up_weight,
    down_weight,
):
    sp = lax.axis_index(("z", "x", "c"))
    at = jnp.stack([lax.axis_index("tp"), lax.axis_index("c")]).astype(jnp.int32)
    query, kv, query_own, kv_own, mix_weights = prepare(
        first_query, second_query, first_key, second_key, values, up_weight, down_weight.T, sp * TOK
    )
    ring = ("z", "c")
    onward = [(2 * z + c, 2 * ((z + 1 - 2 * c) % 8) + c) for z in range(8) for c in range(2)]
    crossed = [(2 * z + c, 2 * ((z - 1 + 2 * c) % 8) + 1 - c) for z in range(8) for c in range(2)]
    near = [lax.ppermute(kv, ring, onward), lax.ppermute(kv, ring, crossed)]
    other = shifted(kv, "c", 1)
    queries = [query_own] + [shifted(query, "x", o) for o in (1, 2, 3)]
    mix_weights = lax.all_gather(mix_weights, ("z", "x", "c"))
    half = lax.dynamic_slice_in_dim(out_weight, lax.axis_index("c") * VD, VD, 0)
    near = jnp.stack(near)
    second = lax.ppermute(near, ring, onward)
    mine = jnp.stack([half] + [shifted(half, "tp", o) for o in (1, 2, 3)])
    out_weights = [mine, shifted(mine, "c", 1)]
    qs, *state = attend_first(queries, kv_own, other)
    third = lax.ppermute(second, ring, onward)
    four = jnp.concatenate([near, second])
    four_other = shifted(four, "c", 1)
    state = attend_next(qs, four, state)
    state = attend_next(qs, four_other, state)
    far = lax.ppermute(third[0], ring, onward)
    third_other = shifted(third, "c", 1)
    state = attend_next(qs, third, state)
    state = attend_next(qs, third_other, state)
    far_other = shifted(far, "c", 1)
    state = attend_last(qs, far, (*state, jnp.zeros((16, TOK), F32)))
    acc, _, tot, lse = attend_last(qs, far_other, state)
    lses = [lse] + [shifted(lse, "x", k) for k in (1, 2, 3)]
    parts = share(lambdas, lses, acc, tot)
    parts = [parts[0]] + [shifted(parts[o], "x", -o) for o in (1, 2, 3)]
    flats = heads(at, head_gain, parts)
    flats = [flats[0]] + [shifted(flats[o], "tp", o) for o in (1, 2, 3)]
    normed = merge(at, flats, residual, norm_gain, out_weights)
    mix_weights = load_mix(mix_weights)
    rows = normed.shape[0] // 2
    before = shifted(normed, "tp", 1)
    after = shifted(normed, "tp", -1)
    cut1 = before[:rows]
    cut3 = after[rows:]
    across1 = shifted(cut1, "tp", 1)
    across3 = shifted(cut3, "tp", -1)
    low0, low1, low3 = mixer([normed, before, after], mix_weights, (F32, BF16, BF16))
    low1 = shifted(low1, "tp", -1)
    low3 = shifted(low3, "tp", 1)
    across = jnp.concatenate([across1, across3])
    (low2,) = mixer([across], mix_weights, (BF16,))
    low2 = shifted(low2, "tp", 2)
    total = normed.astype(F32) + low0
    for low in (low1, low2, low3):
        total = total + low.astype(F32)
    return total.astype(BF16)


def solution(mesh):
    fine = Mesh(mesh.devices.reshape(8, 4, 2, 4), ("z", "x", "c", "tp"))
    sp = ("z", "x", "c")
    in_specs = (
        P(sp + ("tp",), None),
        P(sp, "tp"),
        P(sp, "tp"),
        P(sp, "tp"),
        P(sp, "tp"),
        P(sp, "tp"),
        P("tp"),
        P(),
        P("tp", None),
        P(),
        P(sp, "tp"),
        P("tp", sp),
    )
    out_specs = P(sp + ("tp",), None)

    return jax.shard_map(local, mesh=fine, in_specs=in_specs, out_specs=out_specs, check_vma=False)
```

```python
import functools

import jax
import jax.numpy as jnp
from jax import lax
from jax.experimental import pallas as pl
from jax.experimental.pallas import tpu as pltpu
from jax.sharding import Mesh, PartitionSpec as P


F32 = jnp.float32
BF16 = jnp.bfloat16
TOK = 256
HEAD = 64
VD = 128
LOG2E = 1.4426950408889634
NT = (((1,), (1,)), ((), ()))
NN = (((1,), (0,)), ((), ()))
HBM = pl.BlockSpec(memory_space=pltpu.HBM)
SMEM = pl.BlockSpec(memory_space=pltpu.SMEM)
VMEM = pl.BlockSpec(memory_space=pltpu.VMEM)


def prep_kernel(
    cos_ref, sin_ref, qa_ref, qb_ref, ka_ref, kb_ref, v_ref, up_ref, down_ref,
    q_out, kv_out, q_own, kv_own, mix_out,
):
    mix_out[0] = up_ref[...]
    mix_out[1] = down_ref[...]
    cos = jnp.concatenate([cos_ref[...]] * 4, axis=1)
    sin = jnp.concatenate([-sin_ref[...], sin_ref[...]] * 2, axis=1)
    lane = lax.broadcasted_iota(jnp.int32, cos.shape, 1)
    front = (lane % HEAD) < HEAD // 2

    def turn(ref):
        x = ref[...].astype(F32)
        other = jnp.where(front, pltpu.roll(x, 128 - 32, 1), pltpu.roll(x, 32, 1))
        return (x * cos + other * sin).astype(BF16)

    q_out[:, 0:128] = turn(qa_ref)
    q_out[:, 128:256] = turn(qb_ref)
    kv_out[0:TOK, 0:128] = turn(ka_ref)
    kv_out[0:TOK, 128:256] = turn(kb_ref)
    kv_out[TOK : 2 * TOK, :] = v_ref[...].astype(F32).T.astype(BF16)
    q_own[...] = q_out[...]
    kv_own[...] = kv_out[...]


def prepare(first_query, second_query, first_key, second_key, values, up, down, start):
    positions = (start + jnp.arange(TOK)).astype(F32)
    half = HEAD // 2
    inverse = 10000.0 ** (-jnp.arange(0, half, dtype=F32) * 2.0 / HEAD)
    angle = positions[:, None] * inverse[None, :]
    cos, sin = jnp.cos(angle), jnp.sin(angle)
    return pl.pallas_call(
        prep_kernel,
        out_shape=(
            jax.ShapeDtypeStruct((TOK, 2 * VD), BF16),
            jax.ShapeDtypeStruct((2 * TOK, 2 * VD), BF16),
        )
        * 2
        + (jax.ShapeDtypeStruct((2,) + up.shape, BF16),),
        in_specs=[VMEM] * 9,
        out_specs=(VMEM,) * 5,
        name="prep",
    )(cos, sin, first_query, second_query, first_key, second_key, values, up, down)


def load_queries(queries, qs):
    lane = lax.broadcasted_iota(jnp.int32, (TOK, 128), 1)
    for o, q in enumerate(queries):
        for m in range(2):
            scaled = q[:, m * 128 : (m + 1) * 128].astype(F32) * (LOG2E * HEAD**-0.5)
            hi = scaled.astype(BF16).astype(F32)
            lo = scaled - hi
            for h in range(2):
                mine = (lane < HEAD) if h == 0 else (lane >= HEAD)
                qs[o, 2 * h + m, :, 0:128] = jnp.where(mine, hi, 0.0).astype(BF16)
                qs[o, 2 * h + m, :, 128:256] = jnp.where(mine, lo, 0.0).astype(BF16)


def absorb(chunks, qs, sc, acc, top, tot, fresh):
    def scores(slot, o, hm):
        m = hm % 2
        keys = jnp.concatenate([c[0:TOK, m * 128 : (m + 1) * 128] for c in chunks], axis=0)
        both = jnp.concatenate([keys, keys], axis=1)
        s = lax.dot_general(both, qs[o, hm], NT, preferred_element_type=F32)
        sc[slot] = s
        return jnp.max(s, axis=0, keepdims=True)

    def step(o, peak):
        after = jnp.minimum(o + 1, 3)
        for hm in range(4):
            here = peak
            peak = scores((hm + 1) % 2, o, hm + 1) if hm < 3 else scores(0, after, 0)
            h = hm // 2
            if fresh:
                new = here
            else:
                old = top[o, hm]
                new = jnp.maximum(old, here)
                shrink = jnp.exp2(old - new)
            p = jnp.exp2(sc[hm % 2] - new)
            vals = jnp.concatenate([c[TOK + h * VD : TOK + (h + 1) * VD, :] for c in chunks], axis=1)
            moved = lax.dot_general(vals, p.astype(BF16), NN, preferred_element_type=F32)
            total = jnp.sum(p, axis=0, keepdims=True)
            top[o, hm] = new
            if fresh:
                tot[o, hm] = total
                acc[o, hm] = moved
            else:
                tot[o, hm] = tot[o, hm] * shrink + total
                acc[o, hm] = acc[o, hm] * shrink + moved
        return peak

    lax.fori_loop(0, 4, step, scores(0, 0, 0))


STATE = (
    jax.ShapeDtypeStruct((4, 4, VD, TOK), F32),
    jax.ShapeDtypeStruct((4, 4, 1, TOK), F32),
    jax.ShapeDtypeStruct((4, 4, 1, TOK), F32),
)
QS = jax.ShapeDtypeStruct((4, 4, TOK, 2 * VD), BF16)


def chunks_of(ref):
    return [ref] if len(ref.shape) == 2 else [ref.at[i] for i in range(ref.shape[0])]


def first_kernel(q0, q1, q2, q3, own_ref, other_ref, qs, acc, top, tot, sc):
    load_queries((q0, q1, q2, q3), qs)
    absorb([own_ref, other_ref], qs, sc, acc, top, tot, True)


def next_kernel(qs, kv_ref, acc_in, top_in, tot_in, acc, top, tot, sc):
    absorb(chunks_of(kv_ref), qs, sc, acc, top, tot, False)


def last_kernel(qs, kv_ref, acc_in, top_in, tot_in, acc, top, tot, lse, sc):
    absorb(chunks_of(kv_ref), qs, sc, acc, top, tot, False)
    for o in range(4):
        for hm in range(4):
            row = 4 * o + hm
            lse[row : row + 1, :] = top[o, hm] + jnp.log2(tot[o, hm])


def share_kernel(x_ref, lam_ref, lse0, lse1, lse2, lse3, acc, tot, out_ref):
    lses = (lse0, lse1, lse2, lse3)
    for o in range(4):
        home = (x_ref[0] + 4 - o) % 4
        factors = []
        for hm in range(4):
            rows = [4 * ((o - k) % 4) + hm for k in range(4)]
            here = [ref[row : row + 1, :] for ref, row in zip(lses, rows)]
            peak = jnp.maximum(jnp.maximum(here[0], here[1]), jnp.maximum(here[2], here[3]))
            terms = [jnp.exp2(e - peak) for e in here]
            factors.append(terms[0] / ((terms[0] + terms[1] + terms[2] + terms[3]) * tot[o, hm]))
        for h in range(2):
            diff = acc[o, 2 * h] * factors[2 * h] - acc[o, 2 * h + 1] * (lam_ref[h] * factors[2 * h + 1])
            out_ref[pl.ds(4 * home, 4), :, h * VD : (h + 1) * VD] = diff.T.astype(BF16).reshape(
                4, TOK // 4, VD
            )


def cost(keys):
    return pl.CostEstimate(
        flops=2 * keys * 4 * TOK * 4 * 3 * HEAD,
        bytes_accessed=keys * 1024,
        transcendentals=keys * 4 * TOK * 4,
    )


def score_scratch(chunks):
    return pltpu.VMEM((2, chunks * TOK, TOK), F32)


def attend_first(queries, own, other):
    return pl.pallas_call(
        first_kernel,
        out_shape=(QS,) + STATE,
        in_specs=[VMEM] * 6,
        out_specs=(VMEM,) * 4,
        scratch_shapes=[score_scratch(2)],
        cost_estimate=cost(512),
        compiler_params=pltpu.CompilerParams(vmem_limit_bytes=24 * 2**20),
        name="attend_first",
    )(*queries, own, other)


def attend_next(qs, kv, state):
    keys = kv.shape[0] * TOK if len(kv.shape) == 3 else kv.shape[0] // 2
    return pl.pallas_call(
        next_kernel,
        out_shape=STATE,
        in_specs=[VMEM] * 5,
        out_specs=(VMEM,) * 3,
        input_output_aliases={2: 0, 3: 1, 4: 2},
        scratch_shapes=[score_scratch(keys // TOK)],
        cost_estimate=cost(keys),
        compiler_params=pltpu.CompilerParams(vmem_limit_bytes=24 * 2**20),
        name="attend_next",
    )(qs, kv, *state)


def attend_last(qs, kv, state):
    return pl.pallas_call(
        last_kernel,
        out_shape=STATE + (jax.ShapeDtypeStruct((16, TOK), F32),),
        in_specs=[VMEM] * 5,
        out_specs=(VMEM,) * 4,
        input_output_aliases={2: 0, 3: 1, 4: 2},
        scratch_shapes=[score_scratch(kv.shape[0])],
        cost_estimate=cost(kv.shape[0] * TOK),
        compiler_params=pltpu.CompilerParams(vmem_limit_bytes=24 * 2**20),
        name="attend_last",
    )(qs, kv, *state)


def share(x, lambdas, lses, acc, tot):
    return pl.pallas_call(
        share_kernel,
        out_shape=jax.ShapeDtypeStruct((16, TOK // 4, 2 * VD), BF16),
        in_specs=[SMEM, SMEM] + [VMEM] * 6,
        out_specs=VMEM,
        compiler_params=pltpu.CompilerParams(vmem_limit_bytes=16 * 2**20),
        name="share",
    )(x, lambdas, *lses, acc, tot)


def load_mix_kernel(w_ref, out_ref, sem):
    cuts = 4
    per = w_ref.shape[0] // cuts
    copies = []
    for i in range(cuts):
        rows = pl.ds(i * per, per)
        copies.append(pltpu.make_async_copy(w_ref.at[rows], out_ref.at[rows], sem.at[i]))
        copies[-1].start()
    for copy in copies:
        copy.wait()


def load_mix(weights):
    return pl.pallas_call(
        load_mix_kernel,
        out_shape=jax.ShapeDtypeStruct(weights.shape, BF16),
        in_specs=[HBM],
        out_specs=VMEM,
        scratch_shapes=[pltpu.SemaphoreType.DMA((4,))],
        compiler_params=pltpu.CompilerParams(vmem_limit_bytes=20 * 2**20),
        name="load_mix",
    )(weights)


def merge_kernel(at_ref, part_ref, gain_ref, res_ref, norm_ref, mine_ref, other_ref, out_ref, wbuf, sem):
    mine = at_ref[1] * VD
    copies = []
    for o in range(4):
        near, far = pl.ds(mine, VD), pl.ds(VD - mine, VD)
        copies.append(
            [
                pltpu.make_async_copy(mine_ref.at[o], wbuf.at[o, near], sem.at[2 * o]),
                pltpu.make_async_copy(other_ref.at[o], wbuf.at[o, far], sem.at[2 * o + 1]),
            ]
        )
    for pair in copies:
        for copy in pair:
            copy.start()
    stream = res_ref[...].astype(F32)
    for o in range(4):
        y = (at_ref[0] + 4 - o) % 4
        both = sum(part_ref[4 * k + y].astype(F32) for k in range(4))
        heads = []
        for h in range(2):
            diff = both[:, h * VD : (h + 1) * VD]
            scale = lax.rsqrt(jnp.mean(diff * diff, axis=-1, keepdims=True) + 1e-05)
            heads.append((diff * scale * gain_ref[...] * 0.8).astype(BF16))
        flat = jnp.concatenate(heads, axis=1)
        for copy in copies[o]:
            copy.wait()
        stream = stream + lax.dot_general(flat, wbuf[o], NN, preferred_element_type=F32)
    center = stream - jnp.mean(stream, axis=-1, keepdims=True)
    spread = jnp.mean(center * center, axis=-1, keepdims=True)
    out_ref[...] = (center * lax.rsqrt(spread + 1e-05) * norm_ref[...]).astype(BF16)


def merge(at, part, head_gain, residual, norm_gain, weights):
    rows, width = residual.shape
    return pl.pallas_call(
        merge_kernel,
        out_shape=jax.ShapeDtypeStruct((rows, width), BF16),
        in_specs=[SMEM] + [VMEM] * 4 + [HBM] * 2,
        out_specs=VMEM,
        scratch_shapes=[pltpu.VMEM((4, 2 * VD, width), BF16), pltpu.SemaphoreType.DMA((8,))],
        compiler_params=pltpu.CompilerParams(vmem_limit_bytes=24 * 2**20),
        name="merge",
    )(at, part, head_gain.reshape(1, VD), residual, norm_gain.reshape(1, width), *weights)


def mixer_kernel(count, *refs):
    pieces, w_ref, outs = refs[:count], refs[count], refs[count + 1 :]
    devices, _, rows, hidden_width = w_ref.shape
    x = jnp.concatenate([n[...] for n in pieces], axis=0)
    cuts = 4
    per = devices // cuts
    step = per * rows
    lifted = None
    for i in range(cuts):
        block = w_ref[i * per : (i + 1) * per, 0].reshape(step, hidden_width)
        more = lax.dot_general(x[:, i * step : (i + 1) * step], block, NN, preferred_element_type=F32)
        lifted = more if lifted is None else lifted + more
    pos = jnp.maximum(lifted, 0.0)
    hidden = (pos * pos).astype(BF16)
    for i in range(cuts):
        block = w_ref[i * per : (i + 1) * per, 1].reshape(step, hidden_width)
        low = lax.dot_general(hidden, block, NT, preferred_element_type=F32)
        at = 0
        for n, o in zip(pieces, outs):
            o[:, i * step : (i + 1) * step] = low[at : at + o.shape[0]].astype(o.dtype)
            at += o.shape[0]


def mixer(pieces, weights, types):
    width = pieces[0].shape[1]
    return pl.pallas_call(
        functools.partial(mixer_kernel, len(pieces)),
        out_shape=[jax.ShapeDtypeStruct(n.shape, t) for n, t in zip(pieces, types)],
        in_specs=[VMEM] * (len(pieces) + 1),
        out_specs=[VMEM] * len(pieces),
        cost_estimate=pl.CostEstimate(flops=2 * 256 * width * 2048, bytes_accessed=2**23, transcendentals=0),
        compiler_params=pltpu.CompilerParams(vmem_limit_bytes=24 * 2**20),
        name="mixer",
    )(*pieces, weights)


def shifted(value, axis, by):
    size = lax.axis_size(axis)
    return lax.ppermute(value, axis, [(i, (i + by) % size) for i in range(size)])


def local(
    residual,
    first_query,
    second_query,
    first_key,
    second_key,
    values,
    lambdas,
    head_gain,
    out_weight,
    norm_gain,
    up_weight,
    down_weight,
):
    sp = lax.axis_index(("z", "x", "c"))
    x = lax.axis_index("x").astype(jnp.int32).reshape(1)
    at = jnp.stack([lax.axis_index("tp"), lax.axis_index("c")]).astype(jnp.int32)
    query, kv, query_own, kv_own, mix_weights = prepare(
        first_query, second_query, first_key, second_key, values, up_weight, down_weight.T, sp * TOK
    )
    ring = ("z", "c")
    onward = [(2 * z + c, 2 * ((z + 1 - 2 * c) % 8) + c) for z in range(8) for c in range(2)]
    crossed = [(2 * z + c, 2 * ((z - 1 + 2 * c) % 8) + 1 - c) for z in range(8) for c in range(2)]
    near = [lax.ppermute(kv, ring, onward), lax.ppermute(kv, ring, crossed)]
    other = shifted(kv, "c", 1)
    queries = [query_own] + [shifted(query, "x", o) for o in (1, 2, 3)]
    mix_weights = lax.all_gather(mix_weights, ("z", "x", "c"))
    half = lax.dynamic_slice_in_dim(out_weight, lax.axis_index("c") * VD, VD, 0)
    near = jnp.stack(near)
    second = lax.ppermute(near, ring, onward)
    mine = jnp.stack([half] + [shifted(half, "tp", o) for o in (1, 2, 3)])
    out_weights = [mine, shifted(mine, "c", 1)]
    qs, *state = attend_first(queries, kv_own, other)
    third = lax.ppermute(second, ring, onward)
    four = jnp.concatenate([near, second])
    four_other = shifted(four, "c", 1)
    state = attend_next(qs, four, state)
    state = attend_next(qs, four_other, state)
    far = lax.ppermute(third, ring, onward)
    third_other = shifted(third, "c", 1)
    state = attend_next(qs, third, state)
    state = attend_next(qs, third_other, state)
    acc, _, tot, lse = attend_last(qs, far, state)
    lses = [lse] + [shifted(lse, "x", k) for k in (1, 2, 3)]
    part = share(x, lambdas, lses, acc, tot)
    part = lax.all_to_all(part, ("x", "tp"), split_axis=0, concat_axis=0, tiled=True)
    normed = merge(at, part, head_gain, residual, norm_gain, out_weights)
    mix_weights = load_mix(mix_weights)
    rows = normed.shape[0] // 2
    before = shifted(normed, "tp", 1)
    after = shifted(normed, "tp", -1)
    cut1 = before[:rows]
    cut3 = after[rows:]
    across1 = shifted(cut1, "tp", 1)
    across3 = shifted(cut3, "tp", -1)
    low0, low1, low3 = mixer([normed, before, after], mix_weights, (F32, BF16, BF16))
    low1 = shifted(low1, "tp", -1)
    low3 = shifted(low3, "tp", 1)
    across = jnp.concatenate([across1, across3])
    (low2,) = mixer([across], mix_weights, (BF16,))
    low2 = shifted(low2, "tp", 2)
    total = normed.astype(F32) + low0
    for low in (low1, low2, low3):
        total = total + low.astype(F32)
    return total.astype(BF16)


def solution(mesh):
    fine = Mesh(mesh.devices.reshape(8, 4, 2, 4), ("z", "x", "c", "tp"))
    sp = ("z", "x", "c")
    in_specs = (
        P(sp + ("tp",), None),
        P(sp, "tp"),
        P(sp, "tp"),
        P(sp, "tp"),
        P(sp, "tp"),
        P(sp, "tp"),
        P("tp"),
        P(),
        P("tp", None),
        P(),
        P(sp, "tp"),
        P("tp", sp),
    )
    out_specs = P(sp + ("tp",), None)

    return jax.shard_map(local, mesh=fine, in_specs=in_specs, out_specs=out_specs, check_vma=False)
```

```python
import functools

import jax
import jax.numpy as jnp
from jax import lax
from jax.experimental import pallas as pl
from jax.experimental.pallas import tpu as pltpu
from jax.sharding import Mesh, PartitionSpec as P


F32 = jnp.float32
BF16 = jnp.bfloat16
TOK = 256
HEAD = 64
VD = 128
LOG2E = 1.4426950408889634
NT = (((1,), (1,)), ((), ()))
NN = (((1,), (0,)), ((), ()))
HBM = pl.BlockSpec(memory_space=pltpu.HBM)
SMEM = pl.BlockSpec(memory_space=pltpu.SMEM)
VMEM = pl.BlockSpec(memory_space=pltpu.VMEM)


def turner(cos_ref, sin_ref):
    cos = jnp.concatenate([cos_ref[...]] * 4, axis=1)
    sin = jnp.concatenate([-sin_ref[...], sin_ref[...]] * 2, axis=1)
    lane = lax.broadcasted_iota(jnp.int32, cos.shape, 1)
    front = (lane % HEAD) < HEAD // 2

    def turn(ref):
        x = ref[...].astype(F32)
        other = jnp.where(front, pltpu.roll(x, 128 - 32, 1), pltpu.roll(x, 32, 1))
        return (x * cos + other * sin).astype(BF16)

    return turn


def prep_keys_kernel(cos_ref, sin_ref, ka_ref, kb_ref, v_ref, up_ref, down_ref, kv_out, kv_own, mix_out):
    mix_out[0] = up_ref[...]
    mix_out[1] = down_ref[...]
    turn = turner(cos_ref, sin_ref)
    kv_out[0:TOK, 0:128] = turn(ka_ref)
    kv_out[0:TOK, 128:256] = turn(kb_ref)
    kv_out[TOK : 2 * TOK, :] = v_ref[...].astype(F32).T.astype(BF16)
    kv_own[...] = kv_out[...]


def prep_queries_kernel(cos_ref, sin_ref, qa_ref, qb_ref, q_out, q_own):
    turn = turner(cos_ref, sin_ref)
    q_out[:, 0:128] = turn(qa_ref)
    q_out[:, 128:256] = turn(qb_ref)
    q_own[...] = q_out[...]


def tables(start):
    positions = (start + jnp.arange(TOK)).astype(F32)
    half = HEAD // 2
    inverse = 10000.0 ** (-jnp.arange(0, half, dtype=F32) * 2.0 / HEAD)
    angle = positions[:, None] * inverse[None, :]
    return jnp.cos(angle), jnp.sin(angle)


def prepare_keys(cos, sin, first_key, second_key, values, up, down):
    kv = jax.ShapeDtypeStruct((2 * TOK, 2 * VD), BF16)
    return pl.pallas_call(
        prep_keys_kernel,
        out_shape=(kv, kv, jax.ShapeDtypeStruct((2,) + up.shape, BF16)),
        in_specs=[VMEM] * 7,
        out_specs=(VMEM,) * 3,
        name="prep_keys",
    )(cos, sin, first_key, second_key, values, up, down)


def prepare_queries(cos, sin, first_query, second_query):
    q = jax.ShapeDtypeStruct((TOK, 2 * VD), BF16)
    return pl.pallas_call(
        prep_queries_kernel,
        out_shape=(q, q),
        in_specs=[VMEM] * 4,
        out_specs=(VMEM,) * 2,
        name="prep_queries",
    )(cos, sin, first_query, second_query)


def load_queries(queries, qs):
    lane = lax.broadcasted_iota(jnp.int32, (TOK, 128), 1)
    for o, q in enumerate(queries):
        for m in range(2):
            scaled = q[:, m * 128 : (m + 1) * 128].astype(F32) * (LOG2E * HEAD**-0.5)
            hi = scaled.astype(BF16).astype(F32)
            lo = scaled - hi
            for h in range(2):
                mine = (lane < HEAD) if h == 0 else (lane >= HEAD)
                qs[o, 2 * h + m, :, 0:128] = jnp.where(mine, hi, 0.0).astype(BF16)
                qs[o, 2 * h + m, :, 128:256] = jnp.where(mine, lo, 0.0).astype(BF16)


def absorb(chunks, qs, sc, acc, top, tot, fresh):
    def scores(slot, o, hm):
        m = hm % 2
        keys = jnp.concatenate([c[0:TOK, m * 128 : (m + 1) * 128] for c in chunks], axis=0)
        both = jnp.concatenate([keys, keys], axis=1)
        s = lax.dot_general(both, qs[o, hm], NT, preferred_element_type=F32)
        sc[slot] = s
        return jnp.max(s, axis=0, keepdims=True)

    def step(o, peak):
        after = jnp.minimum(o + 1, 3)
        for hm in range(4):
            here = peak
            peak = scores((hm + 1) % 2, o, hm + 1) if hm < 3 else scores(0, after, 0)
            h = hm // 2
            if fresh:
                new = here
            else:
                old = top[o, hm]
                new = jnp.maximum(old, here)
                shrink = jnp.exp2(old - new)
            p = jnp.exp2(sc[hm % 2] - new)
            vals = jnp.concatenate([c[TOK + h * VD : TOK + (h + 1) * VD, :] for c in chunks], axis=1)
            moved = lax.dot_general(vals, p.astype(BF16), NN, preferred_element_type=F32)
            total = jnp.sum(p, axis=0, keepdims=True)
            top[o, hm] = new
            if fresh:
                tot[o, hm] = total
                acc[o, hm] = moved
            else:
                tot[o, hm] = tot[o, hm] * shrink + total
                acc[o, hm] = acc[o, hm] * shrink + moved
        return peak

    lax.fori_loop(0, 4, step, scores(0, 0, 0))


STATE = (
    jax.ShapeDtypeStruct((4, 4, VD, TOK), F32),
    jax.ShapeDtypeStruct((4, 4, 1, TOK), F32),
    jax.ShapeDtypeStruct((4, 4, 1, TOK), F32),
)
QS = jax.ShapeDtypeStruct((4, 4, TOK, 2 * VD), BF16)


def chunks_of(ref):
    return [ref] if len(ref.shape) == 2 else [ref.at[i] for i in range(ref.shape[0])]


def first_kernel(q0, q1, q2, q3, own_ref, other_ref, qs, acc, top, tot, sc):
    load_queries((q0, q1, q2, q3), qs)
    absorb([own_ref, other_ref], qs, sc, acc, top, tot, True)


def next_kernel(qs, kv_ref, acc_in, top_in, tot_in, acc, top, tot, sc):
    absorb(chunks_of(kv_ref), qs, sc, acc, top, tot, False)


def last_kernel(qs, kv_ref, acc_in, top_in, tot_in, acc, top, tot, lse, sc):
    absorb(chunks_of(kv_ref), qs, sc, acc, top, tot, False)
    for o in range(4):
        for hm in range(4):
            row = 4 * o + hm
            lse[row : row + 1, :] = top[o, hm] + jnp.log2(tot[o, hm])


def share_kernel(x_ref, lam_ref, lse0, lse1, lse2, lse3, acc, tot, out_ref):
    lses = (lse0, lse1, lse2, lse3)
    for o in range(4):
        home = (x_ref[0] + 4 - o) % 4
        factors = []
        for hm in range(4):
            rows = [4 * ((o - k) % 4) + hm for k in range(4)]
            here = [ref[row : row + 1, :] for ref, row in zip(lses, rows)]
            peak = jnp.maximum(jnp.maximum(here[0], here[1]), jnp.maximum(here[2], here[3]))
            terms = [jnp.exp2(e - peak) for e in here]
            factors.append(terms[0] / ((terms[0] + terms[1] + terms[2] + terms[3]) * tot[o, hm]))
        for h in range(2):
            diff = acc[o, 2 * h] * factors[2 * h] - acc[o, 2 * h + 1] * (lam_ref[h] * factors[2 * h + 1])
            out_ref[pl.ds(4 * home, 4), :, h * VD : (h + 1) * VD] = diff.T.astype(BF16).reshape(
                4, TOK // 4, VD
            )


def cost(keys):
    return pl.CostEstimate(
        flops=2 * keys * 4 * TOK * 4 * 3 * HEAD,
        bytes_accessed=keys * 1024,
        transcendentals=keys * 4 * TOK * 4,
    )


def score_scratch(chunks):
    return pltpu.VMEM((2, chunks * TOK, TOK), F32)


def attend_first(queries, own, other):
    return pl.pallas_call(
        first_kernel,
        out_shape=(QS,) + STATE,
        in_specs=[VMEM] * 6,
        out_specs=(VMEM,) * 4,
        scratch_shapes=[score_scratch(2)],
        cost_estimate=cost(512),
        compiler_params=pltpu.CompilerParams(vmem_limit_bytes=24 * 2**20),
        name="attend_first",
    )(*queries, own, other)


def attend_next(qs, kv, state):
    keys = kv.shape[0] * TOK if len(kv.shape) == 3 else kv.shape[0] // 2
    return pl.pallas_call(
        next_kernel,
        out_shape=STATE,
        in_specs=[VMEM] * 5,
        out_specs=(VMEM,) * 3,
        input_output_aliases={2: 0, 3: 1, 4: 2},
        scratch_shapes=[score_scratch(keys // TOK)],
        cost_estimate=cost(keys),
        compiler_params=pltpu.CompilerParams(vmem_limit_bytes=24 * 2**20),
        name="attend_next",
    )(qs, kv, *state)


def attend_last(qs, kv, state):
    return pl.pallas_call(
        last_kernel,
        out_shape=STATE + (jax.ShapeDtypeStruct((16, TOK), F32),),
        in_specs=[VMEM] * 5,
        out_specs=(VMEM,) * 4,
        input_output_aliases={2: 0, 3: 1, 4: 2},
        scratch_shapes=[score_scratch(kv.shape[0])],
        cost_estimate=cost(kv.shape[0] * TOK),
        compiler_params=pltpu.CompilerParams(vmem_limit_bytes=24 * 2**20),
        name="attend_last",
    )(qs, kv, *state)


def share(x, lambdas, lses, acc, tot):
    return pl.pallas_call(
        share_kernel,
        out_shape=jax.ShapeDtypeStruct((16, TOK // 4, 2 * VD), BF16),
        in_specs=[SMEM, SMEM] + [VMEM] * 6,
        out_specs=VMEM,
        compiler_params=pltpu.CompilerParams(vmem_limit_bytes=16 * 2**20),
        name="share",
    )(x, lambdas, *lses, acc, tot)


def load_mix_kernel(w_ref, out_ref, sem):
    cuts = 4
    per = w_ref.shape[0] // cuts
    copies = []
    for i in range(cuts):
        rows = pl.ds(i * per, per)
        copies.append(pltpu.make_async_copy(w_ref.at[rows], out_ref.at[rows], sem.at[i]))
        copies[-1].start()
    for copy in copies:
        copy.wait()


def load_mix(weights):
    return pl.pallas_call(
        load_mix_kernel,
        out_shape=jax.ShapeDtypeStruct(weights.shape, BF16),
        in_specs=[HBM],
        out_specs=VMEM,
        scratch_shapes=[pltpu.SemaphoreType.DMA((4,))],
        compiler_params=pltpu.CompilerParams(vmem_limit_bytes=20 * 2**20),
        name="load_mix",
    )(weights)


def merge_kernel(at_ref, part_ref, gain_ref, res_ref, norm_ref, mine_ref, other_ref, out_ref, wbuf, sem):
    mine = at_ref[1] * VD
    copies = []
    for o in range(4):
        near, far = pl.ds(mine, VD), pl.ds(VD - mine, VD)
        copies.append(
            [
                pltpu.make_async_copy(mine_ref.at[o], wbuf.at[o, near], sem.at[2 * o]),
                pltpu.make_async_copy(other_ref.at[o], wbuf.at[o, far], sem.at[2 * o + 1]),
            ]
        )
    for pair in copies:
        for copy in pair:
            copy.start()
    stream = res_ref[...].astype(F32)
    for o in range(4):
        y = (at_ref[0] + 4 - o) % 4
        both = sum(part_ref[4 * k + y].astype(F32) for k in range(4))
        heads = []
        for h in range(2):
            diff = both[:, h * VD : (h + 1) * VD]
            scale = lax.rsqrt(jnp.mean(diff * diff, axis=-1, keepdims=True) + 1e-05)
            heads.append((diff * scale * gain_ref[...] * 0.8).astype(BF16))
        flat = jnp.concatenate(heads, axis=1)
        for copy in copies[o]:
            copy.wait()
        stream = stream + lax.dot_general(flat, wbuf[o], NN, preferred_element_type=F32)
    center = stream - jnp.mean(stream, axis=-1, keepdims=True)
    spread = jnp.mean(center * center, axis=-1, keepdims=True)
    out_ref[...] = (center * lax.rsqrt(spread + 1e-05) * norm_ref[...]).astype(BF16)


def merge(at, part, head_gain, residual, norm_gain, weights):
    rows, width = residual.shape
    return pl.pallas_call(
        merge_kernel,
        out_shape=jax.ShapeDtypeStruct((rows, width), BF16),
        in_specs=[SMEM] + [VMEM] * 4 + [HBM] * 2,
        out_specs=VMEM,
        scratch_shapes=[pltpu.VMEM((4, 2 * VD, width), BF16), pltpu.SemaphoreType.DMA((8,))],
        compiler_params=pltpu.CompilerParams(vmem_limit_bytes=24 * 2**20),
        name="merge",
    )(at, part, head_gain.reshape(1, VD), residual, norm_gain.reshape(1, width), *weights)


def mixer_kernel(count, *refs):
    pieces, w_ref, outs = refs[:count], refs[count], refs[count + 1 :]
    devices, _, rows, hidden_width = w_ref.shape
    x = jnp.concatenate([n[...] for n in pieces], axis=0)
    cuts = 4
    per = devices // cuts
    step = per * rows
    lifted = None
    for i in range(cuts):
        block = w_ref[i * per : (i + 1) * per, 0].reshape(step, hidden_width)
        more = lax.dot_general(x[:, i * step : (i + 1) * step], block, NN, preferred_element_type=F32)
        lifted = more if lifted is None else lifted + more
    pos = jnp.maximum(lifted, 0.0)
    hidden = (pos * pos).astype(BF16)
    for i in range(cuts):
        block = w_ref[i * per : (i + 1) * per, 1].reshape(step, hidden_width)
        low = lax.dot_general(hidden, block, NT, preferred_element_type=F32)
        at = 0
        for n, o in zip(pieces, outs):
            o[:, i * step : (i + 1) * step] = low[at : at + o.shape[0]].astype(o.dtype)
            at += o.shape[0]


def mixer(pieces, weights, types):
    width = pieces[0].shape[1]
    return pl.pallas_call(
        functools.partial(mixer_kernel, len(pieces)),
        out_shape=[jax.ShapeDtypeStruct(n.shape, t) for n, t in zip(pieces, types)],
        in_specs=[VMEM] * (len(pieces) + 1),
        out_specs=[VMEM] * len(pieces),
        cost_estimate=pl.CostEstimate(flops=2 * 256 * width * 2048, bytes_accessed=2**23, transcendentals=0),
        compiler_params=pltpu.CompilerParams(vmem_limit_bytes=24 * 2**20),
        name="mixer",
    )(*pieces, weights)


def shifted(value, axis, by):
    size = lax.axis_size(axis)
    return lax.ppermute(value, axis, [(i, (i + by) % size) for i in range(size)])


def local(
    residual,
    first_query,
    second_query,
    first_key,
    second_key,
    values,
    lambdas,
    head_gain,
    out_weight,
    norm_gain,
    up_weight,
    down_weight,
):
    sp = lax.axis_index(("z", "x", "c"))
    x = lax.axis_index("x").astype(jnp.int32).reshape(1)
    at = jnp.stack([lax.axis_index("tp"), lax.axis_index("c")]).astype(jnp.int32)
    cos, sin = tables(sp * TOK)
    kv, kv_own, mix_weights = prepare_keys(
        cos, sin, first_key, second_key, values, up_weight, down_weight.T
    )
    query, query_own = prepare_queries(cos, sin, first_query, second_query)
    ring = ("z", "c")
    onward = [(2 * z + c, 2 * ((z + 1 - 2 * c) % 8) + c) for z in range(8) for c in range(2)]
    crossed = [(2 * z + c, 2 * ((z - 1 + 2 * c) % 8) + 1 - c) for z in range(8) for c in range(2)]
    near = [lax.ppermute(kv, ring, onward), lax.ppermute(kv, ring, crossed)]
    other = shifted(kv, "c", 1)
    queries = [query_own] + [shifted(query, "x", o) for o in (1, 2, 3)]
    mix_weights = lax.all_gather(mix_weights, ("z", "x", "c"))
    half = lax.dynamic_slice_in_dim(out_weight, lax.axis_index("c") * VD, VD, 0)
    near = jnp.stack(near)
    second = lax.ppermute(near, ring, onward)
    mine = jnp.stack([half] + [shifted(half, "tp", o) for o in (1, 2, 3)])
    out_weights = [mine, shifted(mine, "c", 1)]
    qs, *state = attend_first(queries, kv_own, other)
    third = lax.ppermute(second, ring, onward)
    four = jnp.concatenate([near, second])
    four_other = shifted(four, "c", 1)
    state = attend_next(qs, four, state)
    state = attend_next(qs, four_other, state)
    far = lax.ppermute(third, ring, onward)
    third_other = shifted(third, "c", 1)
    state = attend_next(qs, third, state)
    state = attend_next(qs, third_other, state)
    acc, _, tot, lse = attend_last(qs, far, state)
    lses = [lse] + [shifted(lse, "x", k) for k in (1, 2, 3)]
    part = share(x, lambdas, lses, acc, tot)
    part = lax.all_to_all(part, ("x", "tp"), split_axis=0, concat_axis=0, tiled=True)
    normed = merge(at, part, head_gain, residual, norm_gain, out_weights)
    mix_weights = load_mix(mix_weights)
    rows = normed.shape[0] // 2
    before = shifted(normed, "tp", 1)
    after = shifted(normed, "tp", -1)
    cut1 = before[:rows]
    cut3 = after[rows:]
    across1 = shifted(cut1, "tp", 1)
    across3 = shifted(cut3, "tp", -1)
    low0, low1, low3 = mixer([normed, before, after], mix_weights, (F32, BF16, BF16))
    low1 = shifted(low1, "tp", -1)
    low3 = shifted(low3, "tp", 1)
    across = jnp.concatenate([across1, across3])
    (low2,) = mixer([across], mix_weights, (BF16,))
    low2 = shifted(low2, "tp", 2)
    total = normed.astype(F32) + low0
    for low in (low1, low2, low3):
        total = total + low.astype(F32)
    return total.astype(BF16)


def solution(mesh):
    fine = Mesh(mesh.devices.reshape(8, 4, 2, 4), ("z", "x", "c", "tp"))
    sp = ("z", "x", "c")
    in_specs = (
        P(sp + ("tp",), None),
        P(sp, "tp"),
        P(sp, "tp"),
        P(sp, "tp"),
        P(sp, "tp"),
        P(sp, "tp"),
        P("tp"),
        P(),
        P("tp", None),
        P(),
        P(sp, "tp"),
        P("tp", sp),
    )
    out_specs = P(sp + ("tp",), None)

    return jax.shard_map(local, mesh=fine, in_specs=in_specs, out_specs=out_specs, check_vma=False)
```

```python
import functools

import jax
import jax.numpy as jnp
from jax import lax
from jax.experimental import pallas as pl
from jax.experimental.pallas import tpu as pltpu
from jax.sharding import Mesh, PartitionSpec as P


F32 = jnp.float32
BF16 = jnp.bfloat16
TOK = 256
HEAD = 64
VD = 128
LOG2E = 1.4426950408889634
NT = (((1,), (1,)), ((), ()))
NN = (((1,), (0,)), ((), ()))
HBM = pl.BlockSpec(memory_space=pltpu.HBM)
SMEM = pl.BlockSpec(memory_space=pltpu.SMEM)
VMEM = pl.BlockSpec(memory_space=pltpu.VMEM)


def turner(cos_ref, sin_ref):
    cos = jnp.concatenate([cos_ref[...]] * 4, axis=1)
    sin = jnp.concatenate([-sin_ref[...], sin_ref[...]] * 2, axis=1)
    lane = lax.broadcasted_iota(jnp.int32, cos.shape, 1)
    front = (lane % HEAD) < HEAD // 2

    def turn(ref):
        x = ref[...].astype(F32)
        other = jnp.where(front, pltpu.roll(x, 128 - 32, 1), pltpu.roll(x, 32, 1))
        return (x * cos + other * sin).astype(BF16)

    return turn


def prep_keys_kernel(cos_ref, sin_ref, ka_ref, kb_ref, v_ref, up_ref, down_ref, kv_out, kv_own, mix_out):
    mix_out[0] = up_ref[...]
    mix_out[1] = down_ref[...]
    turn = turner(cos_ref, sin_ref)
    kv_out[0:TOK, 0:128] = turn(ka_ref)
    kv_out[0:TOK, 128:256] = turn(kb_ref)
    kv_out[TOK : 2 * TOK, :] = v_ref[...].astype(F32).T.astype(BF16)
    kv_own[...] = kv_out[...]


def prep_queries_kernel(cos_ref, sin_ref, qa_ref, qb_ref, q_out, q_own):
    turn = turner(cos_ref, sin_ref)
    q_out[:, 0:128] = turn(qa_ref)
    q_out[:, 128:256] = turn(qb_ref)
    q_own[...] = q_out[...]


def tables(start):
    positions = (start + jnp.arange(TOK)).astype(F32)
    half = HEAD // 2
    inverse = 10000.0 ** (-jnp.arange(0, half, dtype=F32) * 2.0 / HEAD)
    angle = positions[:, None] * inverse[None, :]
    return jnp.cos(angle), jnp.sin(angle)


def prepare_keys(cos, sin, first_key, second_key, values, up, down):
    kv = jax.ShapeDtypeStruct((2 * TOK, 2 * VD), BF16)
    return pl.pallas_call(
        prep_keys_kernel,
        out_shape=(kv, kv, jax.ShapeDtypeStruct((2,) + up.shape, BF16)),
        in_specs=[VMEM] * 7,
        out_specs=(VMEM,) * 3,
        name="prep_keys",
    )(cos, sin, first_key, second_key, values, up, down)


def prepare_queries(cos, sin, first_query, second_query):
    q = jax.ShapeDtypeStruct((TOK, 2 * VD), BF16)
    return pl.pallas_call(
        prep_queries_kernel,
        out_shape=(q, q),
        in_specs=[VMEM] * 4,
        out_specs=(VMEM,) * 2,
        name="prep_queries",
    )(cos, sin, first_query, second_query)


def load_queries(queries, qs):
    lane = lax.broadcasted_iota(jnp.int32, (TOK, 128), 1)
    for o, q in enumerate(queries):
        for m in range(2):
            scaled = q[:, m * 128 : (m + 1) * 128].astype(F32) * (LOG2E * HEAD**-0.5)
            hi = scaled.astype(BF16).astype(F32)
            lo = scaled - hi
            for h in range(2):
                mine = (lane < HEAD) if h == 0 else (lane >= HEAD)
                qs[o, 2 * h + m, :, 0:128] = jnp.where(mine, hi, 0.0).astype(BF16)
                qs[o, 2 * h + m, :, 128:256] = jnp.where(mine, lo, 0.0).astype(BF16)


def absorb(chunks, qs, sc, acc, top, tot, fresh):
    def scores(slot, o, hm):
        m = hm % 2
        keys = jnp.concatenate([c[0:TOK, m * 128 : (m + 1) * 128] for c in chunks], axis=0)
        both = jnp.concatenate([keys, keys], axis=1)
        s = lax.dot_general(both, qs[o, hm], NT, preferred_element_type=F32)
        sc[slot] = s
        return jnp.max(s, axis=0, keepdims=True)

    def step(o, peak):
        after = jnp.minimum(o + 1, 3)
        for hm in range(4):
            here = peak
            peak = scores((hm + 1) % 2, o, hm + 1) if hm < 3 else scores(0, after, 0)
            h = hm // 2
            if fresh:
                new = here
            else:
                old = top[o, hm]
                new = jnp.maximum(old, here)
                shrink = jnp.exp2(old - new)
            p = jnp.exp2(sc[hm % 2] - new)
            vals = jnp.concatenate([c[TOK + h * VD : TOK + (h + 1) * VD, :] for c in chunks], axis=1)
            moved = lax.dot_general(vals, p.astype(BF16), NN, preferred_element_type=F32)
            total = jnp.sum(p, axis=0, keepdims=True)
            top[o, hm] = new
            if fresh:
                tot[o, hm] = total
                acc[o, hm] = moved
            else:
                tot[o, hm] = tot[o, hm] * shrink + total
                acc[o, hm] = acc[o, hm] * shrink + moved
        return peak

    lax.fori_loop(0, 4, step, scores(0, 0, 0))


STATE = (
    jax.ShapeDtypeStruct((4, 4, VD, TOK), F32),
    jax.ShapeDtypeStruct((4, 4, 1, TOK), F32),
    jax.ShapeDtypeStruct((4, 4, 1, TOK), F32),
)
QS = jax.ShapeDtypeStruct((4, 4, TOK, 2 * VD), BF16)


def chunks_of(ref):
    return [ref] if len(ref.shape) == 2 else [ref.at[i] for i in range(ref.shape[0])]


def first_kernel(q0, q1, q2, q3, own_ref, other_ref, qs, acc, top, tot, sc):
    load_queries((q0, q1, q2, q3), qs)
    absorb([own_ref, other_ref], qs, sc, acc, top, tot, True)


def next_kernel(qs, kv_ref, acc_in, top_in, tot_in, acc, top, tot, sc):
    absorb(chunks_of(kv_ref), qs, sc, acc, top, tot, False)


def last_kernel(qs, kv_ref, acc_in, top_in, tot_in, acc, top, tot, lse, sc):
    absorb(chunks_of(kv_ref), qs, sc, acc, top, tot, False)
    for o in range(4):
        for hm in range(4):
            row = 4 * o + hm
            lse[row : row + 1, :] = top[o, hm] + jnp.log2(tot[o, hm])


def share_kernel(x_ref, lam_ref, lse0, lse1, lse2, lse3, acc, tot, out_ref):
    lses = (lse0, lse1, lse2, lse3)
    for o in range(4):
        home = (x_ref[0] + 4 - o) % 4
        factors = []
        for hm in range(4):
            rows = [4 * ((o - k) % 4) + hm for k in range(4)]
            here = [ref[row : row + 1, :] for ref, row in zip(lses, rows)]
            peak = jnp.maximum(jnp.maximum(here[0], here[1]), jnp.maximum(here[2], here[3]))
            terms = [jnp.exp2(e - peak) for e in here]
            factors.append(terms[0] / ((terms[0] + terms[1] + terms[2] + terms[3]) * tot[o, hm]))
        for h in range(2):
            diff = acc[o, 2 * h] * factors[2 * h] - acc[o, 2 * h + 1] * (lam_ref[h] * factors[2 * h + 1])
            block = diff.T.astype(BF16).reshape(4, TOK // 4, VD)
            for y in range(4):
                out_ref[4 * y + home, :, h * VD : (h + 1) * VD] = block[y]


def cost(keys):
    return pl.CostEstimate(
        flops=2 * keys * 4 * TOK * 4 * 3 * HEAD,
        bytes_accessed=keys * 1024,
        transcendentals=keys * 4 * TOK * 4,
    )


def score_scratch(chunks):
    return pltpu.VMEM((2, chunks * TOK, TOK), F32)


def attend_first(queries, own, other):
    return pl.pallas_call(
        first_kernel,
        out_shape=(QS,) + STATE,
        in_specs=[VMEM] * 6,
        out_specs=(VMEM,) * 4,
        scratch_shapes=[score_scratch(2)],
        cost_estimate=cost(512),
        compiler_params=pltpu.CompilerParams(vmem_limit_bytes=24 * 2**20),
        name="attend_first",
    )(*queries, own, other)


def attend_next(qs, kv, state):
    keys = kv.shape[0] * TOK if len(kv.shape) == 3 else kv.shape[0] // 2
    return pl.pallas_call(
        next_kernel,
        out_shape=STATE,
        in_specs=[VMEM] * 5,
        out_specs=(VMEM,) * 3,
        input_output_aliases={2: 0, 3: 1, 4: 2},
        scratch_shapes=[score_scratch(keys // TOK)],
        cost_estimate=cost(keys),
        compiler_params=pltpu.CompilerParams(vmem_limit_bytes=24 * 2**20),
        name="attend_next",
    )(qs, kv, *state)


def attend_last(qs, kv, state):
    return pl.pallas_call(
        last_kernel,
        out_shape=STATE + (jax.ShapeDtypeStruct((16, TOK), F32),),
        in_specs=[VMEM] * 5,
        out_specs=(VMEM,) * 4,
        input_output_aliases={2: 0, 3: 1, 4: 2},
        scratch_shapes=[score_scratch(kv.shape[0])],
        cost_estimate=cost(kv.shape[0] * TOK),
        compiler_params=pltpu.CompilerParams(vmem_limit_bytes=24 * 2**20),
        name="attend_last",
    )(qs, kv, *state)


def share(x, lambdas, lses, acc, tot):
    return pl.pallas_call(
        share_kernel,
        out_shape=jax.ShapeDtypeStruct((16, TOK // 4, 2 * VD), BF16),
        in_specs=[SMEM, SMEM] + [VMEM] * 6,
        out_specs=VMEM,
        compiler_params=pltpu.CompilerParams(vmem_limit_bytes=16 * 2**20),
        name="share",
    )(x, lambdas, *lses, acc, tot)


def load_mix_kernel(w_ref, out_ref, sem):
    cuts = 4
    per = w_ref.shape[0] // cuts
    copies = []
    for i in range(cuts):
        rows = pl.ds(i * per, per)
        copies.append(pltpu.make_async_copy(w_ref.at[rows], out_ref.at[rows], sem.at[i]))
        copies[-1].start()
    for copy in copies:
        copy.wait()


def load_mix(weights):
    return pl.pallas_call(
        load_mix_kernel,
        out_shape=jax.ShapeDtypeStruct(weights.shape, BF16),
        in_specs=[HBM],
        out_specs=VMEM,
        scratch_shapes=[pltpu.SemaphoreType.DMA((4,))],
        compiler_params=pltpu.CompilerParams(vmem_limit_bytes=20 * 2**20),
        name="load_mix",
    )(weights)


def merge_kernel(at_ref, part_ref, gain_ref, res_ref, norm_ref, mine_ref, other_ref, out_ref, wbuf, sem):
    mine = at_ref[1] * VD
    copies = []
    for o in range(4):
        near, far = pl.ds(mine, VD), pl.ds(VD - mine, VD)
        copies.append(
            [
                pltpu.make_async_copy(mine_ref.at[o], wbuf.at[o, near], sem.at[2 * o]),
                pltpu.make_async_copy(other_ref.at[o], wbuf.at[o, far], sem.at[2 * o + 1]),
            ]
        )
    for pair in copies:
        for copy in pair:
            copy.start()
    stream = res_ref[...].astype(F32)
    for o in range(4):
        y = (at_ref[0] + 4 - o) % 4
        both = sum(part_ref[4 * y + k].astype(F32) for k in range(4))
        heads = []
        for h in range(2):
            diff = both[:, h * VD : (h + 1) * VD]
            scale = lax.rsqrt(jnp.mean(diff * diff, axis=-1, keepdims=True) + 1e-05)
            heads.append((diff * scale * gain_ref[...] * 0.8).astype(BF16))
        flat = jnp.concatenate(heads, axis=1)
        for copy in copies[o]:
            copy.wait()
        stream = stream + lax.dot_general(flat, wbuf[o], NN, preferred_element_type=F32)
    center = stream - jnp.mean(stream, axis=-1, keepdims=True)
    spread = jnp.mean(center * center, axis=-1, keepdims=True)
    out_ref[...] = (center * lax.rsqrt(spread + 1e-05) * norm_ref[...]).astype(BF16)


def merge(at, part, head_gain, residual, norm_gain, weights):
    rows, width = residual.shape
    return pl.pallas_call(
        merge_kernel,
        out_shape=jax.ShapeDtypeStruct((rows, width), BF16),
        in_specs=[SMEM] + [VMEM] * 4 + [HBM] * 2,
        out_specs=VMEM,
        scratch_shapes=[pltpu.VMEM((4, 2 * VD, width), BF16), pltpu.SemaphoreType.DMA((8,))],
        compiler_params=pltpu.CompilerParams(vmem_limit_bytes=24 * 2**20),
        name="merge",
    )(at, part, head_gain.reshape(1, VD), residual, norm_gain.reshape(1, width), *weights)


def mixer_kernel(count, *refs):
    pieces, w_ref, outs = refs[:count], refs[count], refs[count + 1 :]
    devices, _, rows, hidden_width = w_ref.shape
    x = jnp.concatenate([n[...] for n in pieces], axis=0)
    cuts = 4
    per = devices // cuts
    step = per * rows
    lifted = None
    for i in range(cuts):
        block = w_ref[i * per : (i + 1) * per, 0].reshape(step, hidden_width)
        more = lax.dot_general(x[:, i * step : (i + 1) * step], block, NN, preferred_element_type=F32)
        lifted = more if lifted is None else lifted + more
    pos = jnp.maximum(lifted, 0.0)
    hidden = (pos * pos).astype(BF16)
    for i in range(cuts):
        block = w_ref[i * per : (i + 1) * per, 1].reshape(step, hidden_width)
        low = lax.dot_general(hidden, block, NT, preferred_element_type=F32)
        at = 0
        for n, o in zip(pieces, outs):
            o[:, i * step : (i + 1) * step] = low[at : at + o.shape[0]].astype(o.dtype)
            at += o.shape[0]


def mixer(pieces, weights, types):
    width = pieces[0].shape[1]
    return pl.pallas_call(
        functools.partial(mixer_kernel, len(pieces)),
        out_shape=[jax.ShapeDtypeStruct(n.shape, t) for n, t in zip(pieces, types)],
        in_specs=[VMEM] * (len(pieces) + 1),
        out_specs=[VMEM] * len(pieces),
        cost_estimate=pl.CostEstimate(flops=2 * 256 * width * 2048, bytes_accessed=2**23, transcendentals=0),
        compiler_params=pltpu.CompilerParams(vmem_limit_bytes=24 * 2**20),
        name="mixer",
    )(*pieces, weights)


def shifted(value, axis, by):
    size = lax.axis_size(axis)
    return lax.ppermute(value, axis, [(i, (i + by) % size) for i in range(size)])


def local(
    residual,
    first_query,
    second_query,
    first_key,
    second_key,
    values,
    lambdas,
    head_gain,
    out_weight,
    norm_gain,
    up_weight,
    down_weight,
):
    sp = lax.axis_index(("z", "x", "c"))
    x = lax.axis_index("x").astype(jnp.int32).reshape(1)
    at = jnp.stack([lax.axis_index("tp"), lax.axis_index("c")]).astype(jnp.int32)
    cos, sin = tables(sp * TOK)
    kv, kv_own, mix_weights = prepare_keys(
        cos, sin, first_key, second_key, values, up_weight, down_weight.T
    )
    query, query_own = prepare_queries(cos, sin, first_query, second_query)
    ring = ("z", "c")
    onward = [(2 * z + c, 2 * ((z + 1 - 2 * c) % 8) + c) for z in range(8) for c in range(2)]
    crossed = [(2 * z + c, 2 * ((z - 1 + 2 * c) % 8) + 1 - c) for z in range(8) for c in range(2)]
    near = [lax.ppermute(kv, ring, onward), lax.ppermute(kv, ring, crossed)]
    other = shifted(kv, "c", 1)
    queries = [query_own] + [shifted(query, "x", o) for o in (1, 2, 3)]
    mix_weights = lax.all_gather(mix_weights, ("z", "x", "c"))
    half = lax.dynamic_slice_in_dim(out_weight, lax.axis_index("c") * VD, VD, 0)
    near = jnp.stack(near)
    second = lax.ppermute(near, ring, onward)
    mine = jnp.stack([half] + [shifted(half, "tp", o) for o in (1, 2, 3)])
    out_weights = [mine, shifted(mine, "c", 1)]
    qs, *state = attend_first(queries, kv_own, other)
    third = lax.ppermute(second, ring, onward)
    four = jnp.concatenate([near, second])
    four_other = shifted(four, "c", 1)
    state = attend_next(qs, four, state)
    state = attend_next(qs, four_other, state)
    far = lax.ppermute(third, ring, onward)
    third_other = shifted(third, "c", 1)
    state = attend_next(qs, third, state)
    state = attend_next(qs, third_other, state)
    acc, _, tot, lse = attend_last(qs, far, state)
    lses = [lse] + [shifted(lse, "x", k) for k in (1, 2, 3)]
    part = share(x, lambdas, lses, acc, tot)
    part = lax.all_to_all(part, ("tp", "x"), split_axis=0, concat_axis=0, tiled=True)
    normed = merge(at, part, head_gain, residual, norm_gain, out_weights)
    mix_weights = load_mix(mix_weights)
    rows = normed.shape[0] // 2
    before = shifted(normed, "tp", 1)
    after = shifted(normed, "tp", -1)
    cut1 = before[:rows]
    cut3 = after[rows:]
    across1 = shifted(cut1, "tp", 1)
    across3 = shifted(cut3, "tp", -1)
    low0, low1, low3 = mixer([normed, before, after], mix_weights, (F32, BF16, BF16))
    low1 = shifted(low1, "tp", -1)
    low3 = shifted(low3, "tp", 1)
    across = jnp.concatenate([across1, across3])
    (low2,) = mixer([across], mix_weights, (BF16,))
    low2 = shifted(low2, "tp", 2)
    total = normed.astype(F32) + low0
    for low in (low1, low2, low3):
        total = total + low.astype(F32)
    return total.astype(BF16)


def solution(mesh):
    fine = Mesh(mesh.devices.reshape(8, 4, 2, 4), ("z", "x", "c", "tp"))
    sp = ("z", "x", "c")
    in_specs = (
        P(sp + ("tp",), None),
        P(sp, "tp"),
        P(sp, "tp"),
        P(sp, "tp"),
        P(sp, "tp"),
        P(sp, "tp"),
        P("tp"),
        P(),
        P("tp", None),
        P(),
        P(sp, "tp"),
        P("tp", sp),
    )
    out_specs = P(sp + ("tp",), None)

    return jax.shard_map(local, mesh=fine, in_specs=in_specs, out_specs=out_specs, check_vma=False)
```
